512 devices in a mesh: row: 64 (over z, y), col: 8 (over x, core).
Axes of the slice: x: 4, y: 4, z: 16, core: 2. Of those that a mesh axis runs over, the one named last changes fastest.
Arguments:
- tokens: bfloat16 [8, 12288, 2048], P('col', 'row'), may hold values from -6 to 6
- proj_in: bfloat16 [2048, 512], P('col'), may hold values from -0.125 to 0.125
- proj_out: bfloat16 [512, 2048], P(None, 'row'), may hold values from -0.25 to 0.25
Outputs:
- output: bfloat16 [8, 12288, 2048], P('col', 'row')
The draws below stay inside these ranges and needn't reach their ends.
All inputs are finite; a program needn't handle non-finite values.
Results may differ from the reference program's by a relative error of at most 0.0083.
Values may be sent and summed in bfloat16 or wider, within the bound.
A program may use at most 64 MiB of HBM per device.

```python
import jax
import jax.numpy as jnp
from jax import lax

D = 2048
GROUPS = 4
GRP = 128
FW = 512
LEN = 12288
BATCH = 8


def steps_of(rng, extent, split, smallest, largest):
    level = 1.0
    for axis_at, shards_of in split:
        draws = jax.random.uniform(jax.random.fold_in(jax.random.fold_in(rng, 6), axis_at), (shards_of,), jnp.float32, smallest / len(split), largest / len(split))
        level = level * jnp.repeat(jnp.exp(draws), extent[axis_at] // shards_of).reshape((-1,) + (1,) * (len(extent) - 1 - axis_at))
    return level


def scatter_about(own_key, shape, spread, reach, pieces=(), kind=jnp.bfloat16):
    gain = steps_of(own_key, shape, pieces, -0.22, 0.18) if pieces else 1.0
    values = jax.random.normal(own_key, shape, jnp.float32) * spread * gain
    return jnp.minimum(jnp.maximum(values, -reach), reach).astype(kind)


def setup_inputs(seed: int = 0) -> dict:
    seeds = jax.random.split(jax.random.key(seed), 4)
    return {
        "tokens": scatter_about(seeds[0], (BATCH, LEN, D), 1.0, 6.0, ((0, 8), (1, 64))),
        "proj_in": scatter_about(seeds[1], (D, FW), D ** -0.5, 0.125, ((0, 8),)),
        "proj_out": scatter_about(seeds[2], (FW, D), FW ** -0.5, 0.25, ((1, 64),)),
    }


def reference(tokens, proj_in, proj_out):
    def one_sequence(seq):
        mapped = jnp.dot(seq, proj_in, preferred_element_type=jnp.float32).astype(jnp.bfloat16)
        length = seq.shape[0]
        grid = mapped.astype(jnp.float32).reshape(length, GROUPS, GRP)
        spectrum = jnp.fft.fft2(grid, axes=(0, 2), norm="ortho").real
        mixed = spectrum.reshape(length, GROUPS * GRP).astype(jnp.bfloat16)
        return jnp.dot(mixed, proj_out, preferred_element_type=jnp.float32).astype(jnp.bfloat16)

    return lax.map(one_sequence, tokens)
```

```python
import math

import jax
import jax.numpy as jnp
import numpy as np
from jax import lax
from jax.experimental import pallas as pl
from jax.experimental.pallas import tpu as pltpu
from jax.sharding import PartitionSpec as P

MESH = pl.DeviceIdType.MESH
GRP = 128
GROUPS = 4
NZ, NY, NX = 16, 4, 4
ROWS = NZ * NY
LOC = 192
LEN = ROWS * LOC
D = 2048
KS = 256
FW = GROUPS * GRP
F32 = jnp.float32
BF = jnp.bfloat16


def tables():
    s = np.arange(64)[:, None]
    f = np.arange(GRP)[None, :]
    ang = 2 * np.pi * ((s * f) % GRP) / GRP
    part_a = np.cos(ang)
    part_b = np.sin(ang)
    part_b[0] = np.cos(np.pi * np.arange(GRP))
    chan = np.concatenate([part_a, part_b], 1)
    q = np.arange(LOC)[:, None]
    p1 = np.arange(LOC)[None, :]
    ang = 2 * np.pi * ((q * p1) % LOC) / LOC
    first = np.repeat(np.concatenate([np.cos(ang), np.sin(ang)], 0), 4, axis=1)
    q2 = np.arange(64)[None, :]
    ang = 2 * np.pi * ((q * q2) % LEN) / LEN
    scale = 1.0 / math.sqrt(GRP * LEN)
    twist = np.stack([np.tile(np.cos(ang), (1, 2)), np.tile(np.sin(ang), (1, 2))]) * scale
    r = np.arange(64)[:, None]
    ang = 2 * np.pi * ((r * q2) % 64) / 64
    c, n = np.cos(ang), np.sin(ang)
    last = np.repeat(np.concatenate([c, n, -n, c], 1), 4, axis=0)
    return chan, first, twist, last


def bdot(a, b):
    return lax.dot_general(a, b, (((1,), (1,)), ((), ())), preferred_element_type=F32)


def kernel(tok_hbm, win_hbm, pout_hbm, chan_hbm, first_hbm, twist_hbm, last_hbm, out_ref, tok, wfull, pblk, chan, first, twist, last, m1, l3, blk, pt, snd, dat, snd2, dat2, pgx, ld, pin_s, pin_r, a1_s, a1_r, a2_s, a2_r, pz_s, pz_r, py_s, py_r, px_s, px_r):
    row = lax.axis_index("row")
    col = lax.axis_index("col")
    z, y = row // NY, lax.rem(row, NY)
    x, core = col // 2, lax.rem(col, 2)
    xr = lax.rem(x + 1, NX)
    xl = lax.rem(x + NX - 1, NX)
    xo = lax.rem(x + 2, NX)
    right, left, mate = xr * 2 + core, xl * 2 + core, x * 2 + (1 - core)

    bar = pltpu.get_barrier_semaphore()

    def greet_row(o, c):
        pl.semaphore_signal(bar, inc=1, device_id={"row": lax.rem(row + o, ROWS)}, device_id_type=MESH)
        return c

    lax.fori_loop(1, ROWS, greet_row, 0)
    for peer in (right, left, mate):
        pl.semaphore_signal(bar, inc=1, device_id={"col": peer}, device_id_type=MESH)

    loads = [
        pltpu.make_async_copy(win_hbm, wfull.at[pl.ds(pl.multiple_of(col * KS, KS), KS), :], ld.at[0]),
        pltpu.make_async_copy(pout_hbm, pblk, ld.at[1]),
        pltpu.make_async_copy(tok_hbm.at[0], tok, ld.at[2]),
        pltpu.make_async_copy(chan_hbm, chan, ld.at[3]),
        pltpu.make_async_copy(first_hbm, first, ld.at[4]),
        pltpu.make_async_copy(last_hbm, last, ld.at[5]),
        pltpu.make_async_copy(twist_hbm, twist, ld.at[6]),
    ]
    for c in loads:
        c.start()

    rid = lax.broadcasted_iota(jnp.int32, (FW, FW), 1)
    fid = lax.broadcasted_iota(jnp.int32, (FW, FW), 0)
    inner = lax.rem(rid, 256)
    slot = (inner // 16) * 4 + lax.rem(inner, 4)
    upper = jnp.where(slot == 0, 64, GRP - slot)
    want = lax.rem(inner // 4, 4) * GRP + jnp.where(rid < 256, slot, upper)
    perm = jnp.where(fid == want, 1.0, 0.0).astype(BF)
    loads[1].wait()
    turned = lax.dot_general(pblk[...], perm, (((0,), (0,)), ((), ())), preferred_element_type=F32).astype(BF)
    blk[...] = turned

    for i in (3, 4, 5, 6):
        loads[i].wait()
    lane = lax.rem(lax.broadcasted_iota(jnp.int32, (2 * LOC, 4 * LOC), 1), 4)
    sub = lax.rem(lax.broadcasted_iota(jnp.int32, (256, 256), 0), 4)
    for s in range(4):
        m1[s] = first[...] * jnp.where(lane == s, 1.0, 0.0).astype(BF)
        l3[s] = last[...] * jnp.where(sub == s, 1.0, 0.0).astype(BF)
    loads[0].wait()
    loads[2].wait()

    pl.semaphore_wait(bar, ROWS - 1 + 3)

    def wtile(c, g, lo=0, n=KS):
        return wfull.at[pl.ds(pl.multiple_of(c * KS + lo, 128), n), pl.ds(pl.multiple_of(g * GRP, GRP), GRP)]

    def push(ref, ss, rs, peer):
        return pltpu.make_async_remote_copy(src_ref=ref, dst_ref=ref, send_sem=ss, recv_sem=rs, device_id={"col": peer}, device_id_type=MESH)

    def pin(t, k, g):
        who = (col, col, col, xl * 2 + core, xr * 2 + core, xl * 2 + core, xr * 2 + core, xo * 2 + core, xo * 2 + core)[k]
        lo = (0, 0, 0, 0, 128, 0, 0, 0, 128)[k]
        n = (KS, KS, KS, 128, 128, KS, KS, 128, 128)[k]
        peer = (right, left, mate, right, left, mate, mate, mate, mate)[k]
        return push(wtile(who, g, lo, n), pin_s.at[t, k], pin_r.at[t, k], peer)

    def pin_arrived(t, k, g):
        n = (KS, KS, KS, 128, 128, KS, KS, 128, 128)[k]
        push(wtile(col, g, 0, n), pin_s.at[t, k], pin_r.at[t, k], mate).wait_recv()

    gs = [lax.rem(y + t, GROUPS) for t in range(GROUPS)]
    for t in range(GROUPS):
        for k in range(3):
            pin(t, k, gs[t]).start()

    half = pl.ds(pl.multiple_of(core * 16, 16), 16)
    quarter = pl.ds(pl.multiple_of(x * GRP, GRP), GRP)
    own = pltpu.make_async_copy(blk.at[half, quarter], pgx.at[row], ld.at[7])
    own.start()

    def pz_send(o, c):
        to = lax.rem(row + NY * o, ROWS)
        pltpu.make_async_remote_copy(src_ref=blk.at[half, quarter], dst_ref=pgx.at[row], send_sem=pz_s, recv_sem=pz_r, device_id={"row": to}, device_id_type=MESH).start()
        return c

    own.wait()

    for t in range(GROUPS):
        g = gs[t]
        pin_arrived(t, 0, g)
        pin(t, 3, g).start()
        pin(t, 5, g).start()
        pin_arrived(t, 1, g)
        pin(t, 4, g).start()
        pin(t, 6, g).start()
        pin_arrived(t, 3, g)
        pin(t, 7, g).start()
        pin_arrived(t, 4, g)
        pin(t, 8, g).start()
        for k in (2, 5, 6, 7, 8):
            pin_arrived(t, k, g)
        w = wfull[:, pl.ds(pl.multiple_of(g * GRP, GRP), GRP)]
        mapped = jnp.dot(tok[...], w, preferred_element_type=F32).astype(BF)
        zero = jnp.zeros((64, GRP), BF)
        parts = []
        for m in range(3):
            piece = mapped[64 * m : 64 * m + 64]
            parts.append(jnp.concatenate([piece, zero], 1))
            parts.append(jnp.concatenate([zero, piece], 1))
        spread = bdot(chan[...], jnp.concatenate(parts, 0))
        for m in range(3):
            snd[t, :, m] = spread[:, GRP * m : GRP * m + GRP].reshape(NZ, 4, GRP).astype(BF)

        def a1_send(o, c, t=t, g=g):
            to = lax.rem(z + o, NZ)
            pltpu.make_async_remote_copy(src_ref=snd.at[t, to], dst_ref=dat.at[row], send_sem=a1_s.at[t], recv_sem=a1_r, device_id={"row": to * NY + g}, device_id_type=MESH).start()
            return c

        if t == 0:
            pltpu.make_async_copy(snd.at[0, z], dat.at[row], a1_r).start()
            lax.fori_loop(1, NZ, a1_send, 0)
        else:
            lax.fori_loop(0, NZ, a1_send, 0)

    lax.fori_loop(1, NZ, pz_send, 0)

    def zpart(yy):
        return pgx.at[pl.ds(0, NZ)]

    pltpu.make_async_copy(pgx.at[pl.ds(0, NZ - 1)], pgx.at[pl.ds(0, NZ - 1)], pz_r).wait()
    for o in range(1, NY):
        yo = lax.rem(y + o, NY)

        def py_send(k, c, yo=yo, o=o):
            pltpu.make_async_remote_copy(src_ref=pgx.at[k * NY + y], dst_ref=pgx.at[k * NY + y], send_sem=py_s.at[o - 1], recv_sem=py_r, device_id={"row": z * NY + yo}, device_id_type=MESH).start()
            return c

        lax.fori_loop(0, NZ, py_send, 0)

    pltpu.make_async_copy(dat, dat, a1_r).wait()
    data = dat[...].reshape(4 * LOC, GRP)
    cc, sn = twist[0], twist[1]
    first_slot = z == 0
    lanes = lax.broadcasted_iota(jnp.int32, (1, GRP), 1) < 64
    sgn = jnp.where(lanes, 1.0, -1.0)
    zero_b = jnp.where(lanes, 1.0, 0.0)
    spec = jnp.where(first_slot, 1.0, 0.0)
    outs = [None] * 3
    for s in range(4):
        got = jnp.dot(m1[s], data, preferred_element_type=F32)
        re, im = got[:LOC], got[LOC:]
        tre = re * cc - im * sn
        tim = re * sn + im * cc
        if s == 0:
            lo_mask = zero_b * spec + sgn * (1.0 - spec)
            up_keep, up_turn = 1.0 - spec, zero_b * spec
            lo_re, lo_im = tre * lo_mask, tim * lo_mask
            up_re = tre * up_keep + pltpu.roll(tre, 64, 1) * up_turn
            up_im = tim * up_keep + pltpu.roll(tim, 64, 1) * up_turn
        else:
            lo_re, lo_im, up_re, up_im = tre * sgn, tim * sgn, tre, tim
        lo = jnp.concatenate([lo_re, lo_im], 1).astype(BF)
        up = jnp.concatenate([up_re, up_im], 1).astype(BF)
        for m in range(3):
            rhs = jnp.concatenate([lo[64 * m : 64 * m + 64], up[64 * m : 64 * m + 64]], 0)
            term = bdot(l3[s], rhs)
            outs[m] = term if outs[m] is None else outs[m] + term
    for m in range(3):
        snd2[:, m] = outs[m].reshape(ROWS, 4, GRP).astype(BF)

    pltpu.make_async_copy(snd2.at[row], dat2.at[row], a2_r).start()

    def a2_send(o, c):
        to = lax.rem(row + o, ROWS)
        pltpu.make_async_remote_copy(src_ref=snd2.at[to], dst_ref=dat2.at[row], send_sem=a2_s, recv_sem=a2_r, device_id={"row": to}, device_id_type=MESH).start()
        return c

    lax.fori_loop(1, ROWS, a2_send, 0)

    pltpu.make_async_copy(pgx.at[pl.ds(0, 3 * NZ)], pgx.at[pl.ds(0, 3 * NZ)], py_r).wait()

    def ptile(c, lo=0, n=ROWS):
        return pt.at[pl.ds(lo, n), pl.ds(pl.multiple_of(lax.rem(c, 2) * 16, 16), 16), pl.ds(pl.multiple_of((c // 2) * GRP, GRP), GRP)]

    mine = pltpu.make_async_copy(pgx, ptile(col), ld.at[8])
    mine.start()
    mine.wait()

    def px(k):
        who = (col, col, col, xl * 2 + core, xr * 2 + core, xl * 2 + core, xr * 2 + core, xo * 2 + core, xo * 2 + core)[k]
        lo = (0, 0, 0, 0, 32, 0, 0, 0, 32)[k]
        n = (64, 64, 64, 32, 32, 64, 64, 32, 32)[k]
        peer = (right, left, mate, right, left, mate, mate, mate, mate)[k]
        return push(ptile(who, lo, n), px_s.at[k], px_r.at[k], peer)

    def px_arrived(k):
        n = (64, 64, 64, 32, 32, 64, 64, 32, 32)[k]
        push(ptile(col, 0, n), px_s.at[k], px_r.at[k], mate).wait_recv()

    for k in range(3):
        px(k).start()
    px_arrived(0)
    px(3).start()
    px(5).start()
    px_arrived(1)
    px(4).start()
    px(6).start()
    px_arrived(3)
    px(7).start()
    px_arrived(4)
    px(8).start()
    for k in (2, 5, 6, 7, 8):
        px_arrived(k)

    pltpu.make_async_copy(dat2, dat2, a2_r).wait()
    sides = []
    for m in range(3):
        t = dat2[:, m].reshape(256, GRP).T
        sides.append(jnp.concatenate([t[:64], t[64:]], 1))
    lhs = jnp.concatenate(sides, 0)
    for n in range(8):
        out_ref[0, :, 256 * n : 256 * n + 256] = bdot(lhs, pt[8 * n : 8 * n + 8].reshape(256, FW)).astype(BF)

    for t in range(GROUPS):
        for k in range(9):
            pin(t, k, gs[t]).wait_send()
        n = NZ - 1 if t == 0 else NZ
        pltpu.make_async_copy(snd.at[t, pl.ds(0, n)], snd.at[t, pl.ds(0, n)], a1_s.at[t]).wait()
    for k in range(9):
        px(k).wait_send()
    pltpu.make_async_copy(pgx.at[pl.ds(0, NZ - 1)], pgx.at[pl.ds(0, NZ - 1)], pz_s).wait()
    for o in range(3):
        pltpu.make_async_copy(pgx.at[pl.ds(0, NZ)], pgx.at[pl.ds(0, NZ)], py_s.at[o]).wait()
    pltpu.make_async_copy(snd2.at[pl.ds(0, ROWS - 1)], snd2.at[pl.ds(0, ROWS - 1)], a2_s).wait()


def shards(tokens, proj_in, proj_out):
    chan, first, twist, last = tables()
    anyspec = pl.BlockSpec(memory_space=pl.ANY)
    dma = pltpu.SemaphoreType.DMA
    return pl.pallas_call(
        kernel,
        out_shape=jax.ShapeDtypeStruct((1, LOC, D), BF),
        in_specs=[anyspec] * 7,
        out_specs=pl.BlockSpec(memory_space=pltpu.VMEM),
        scratch_shapes=[
            pltpu.VMEM((LOC, D), BF),
            pltpu.VMEM((D, FW), BF),
            pltpu.VMEM((FW, 32), BF),
            pltpu.VMEM((64, 256), BF),
            pltpu.VMEM((2 * LOC, 4 * LOC), BF),
            pltpu.VMEM((2, LOC, GRP), F32),
            pltpu.VMEM((256, 256), BF),
            pltpu.VMEM((4, 2 * LOC, 4 * LOC), BF),
            pltpu.VMEM((4, 256, 256), BF),
            pltpu.VMEM((32, FW), BF),
            pltpu.VMEM((ROWS, 32, FW), BF),
            pltpu.VMEM((GROUPS, NZ, 3, 4, GRP), BF),
            pltpu.VMEM((ROWS, 3, 4, GRP), BF),
            pltpu.VMEM((ROWS, 3, 4, GRP), BF),
            pltpu.VMEM((ROWS, 3, 4, GRP), BF),
            pltpu.VMEM((ROWS, 16, GRP), BF),
            dma((9,)),
            dma((GROUPS, 9)),
            dma((GROUPS, 9)),
            dma((GROUPS,)),
            dma,
            dma,
            dma,
            dma,
            dma,
            dma((3,)),
            dma,
            dma((9,)),
            dma((9,)),
        ],
        compiler_params=pltpu.CompilerParams(collective_id=0, has_side_effects=True),
    )(
        tokens,
        proj_in,
        proj_out,
        jnp.asarray(chan, BF),
        jnp.asarray(first, BF),
        jnp.asarray(twist, F32),
        jnp.asarray(last, BF),
    )


def solution(mesh):
    return jax.shard_map(
        shards,
        mesh=mesh,
        in_specs=(P("col", "row", None), P("col", None), P(None, "row")),
        out_specs=P("col", "row", None),
        check_vma=False,
    )
```

```python
import math

import jax
import jax.numpy as jnp
import numpy as np
from jax import lax
from jax.experimental import pallas as pl
from jax.experimental.pallas import tpu as pltpu
from jax.sharding import PartitionSpec as P

MESH = pl.DeviceIdType.MESH
GRP = 128
GROUPS = 4
NZ, NY, NX = 16, 4, 4
ROWS = NZ * NY
LOC = 192
LEN = ROWS * LOC
D = 2048
KS = 256
FW = GROUPS * GRP
F32 = jnp.float32
BF = jnp.bfloat16


def tables():
    s = np.arange(64)[:, None]
    f = np.arange(GRP)[None, :]
    ang = 2 * np.pi * ((s * f) % GRP) / GRP
    part_a = np.cos(ang)
    part_b = np.sin(ang)
    part_b[0] = np.cos(np.pi * np.arange(GRP))
    chan = np.concatenate([part_a, part_b], 1)
    q = np.arange(LOC)[:, None]
    p1 = np.arange(LOC)[None, :]
    ang = 2 * np.pi * ((q * p1) % LOC) / LOC
    first = np.repeat(np.concatenate([np.cos(ang), np.sin(ang)], 0), 4, axis=1)
    q2 = np.arange(64)[None, :]
    ang = 2 * np.pi * ((q * q2) % LEN) / LEN
    scale = 1.0 / math.sqrt(GRP * LEN)
    twist = np.stack([np.tile(np.cos(ang), (1, 2)), np.tile(np.sin(ang), (1, 2))]) * scale
    r = np.arange(64)[:, None]
    ang = 2 * np.pi * ((r * q2) % 64) / 64
    c, n = np.cos(ang), np.sin(ang)
    last = np.repeat(np.concatenate([c, n, -n, c], 1), 4, axis=0)
    return chan, first, twist, last


def bdot(a, b):
    return lax.dot_general(a, b, (((1,), (1,)), ((), ())), preferred_element_type=F32)


def kernel(tok_hbm, win_hbm, pout_hbm, chan_hbm, first_hbm, twist_hbm, last_hbm, out_ref, tok, wfull, pblk, chan, first, twist, last, m1, l3, blk, pt, snd, dat, snd2, dat2, pgx, ld, hops, pin_s, pin_r, yin_s, yin_r, ymt_s, ymt_r, a1_s, a1_r, a2_s, a2_r, pz_s, pz_r, py_s, py_r, px_s, px_r):
    row = lax.axis_index("row")
    col = lax.axis_index("col")
    z, y = row // NY, lax.rem(row, NY)
    x, core = col // 2, lax.rem(col, 2)
    xr = lax.rem(x + 1, NX)
    xl = lax.rem(x + NX - 1, NX)
    xo = lax.rem(x + 2, NX)
    right, left, mate = xr * 2 + core, xl * 2 + core, x * 2 + (1 - core)
    yu, yd, yo = lax.rem(y + 1, NY), lax.rem(y + NY - 1, NY), lax.rem(y + 2, NY)

    def at(dz, yy):
        return lax.rem(z + dz, NZ) * NY + yy

    bar = pltpu.get_barrier_semaphore()
    for peer in (right, left, mate):
        pl.semaphore_signal(bar, inc=1, device_id={"col": peer}, device_id_type=MESH)
    for peer in (at(0, yu), at(0, yd), at(1, y), at(NZ - 1, y)):
        pl.semaphore_signal(bar, inc=1, device_id={"row": peer}, device_id_type=MESH)

    loads = [
        pltpu.make_async_copy(win_hbm, wfull.at[pl.ds(pl.multiple_of(col * KS, KS), KS), :], ld.at[0]),
        pltpu.make_async_copy(pout_hbm, pblk, ld.at[1]),
        pltpu.make_async_copy(tok_hbm.at[0], tok, ld.at[2]),
        pltpu.make_async_copy(chan_hbm, chan, ld.at[3]),
        pltpu.make_async_copy(first_hbm, first, ld.at[4]),
        pltpu.make_async_copy(last_hbm, last, ld.at[5]),
        pltpu.make_async_copy(twist_hbm, twist, ld.at[6]),
    ]
    for c in loads:
        c.start()
    loads[0].wait()
    pl.semaphore_wait(bar, 7)

    same = [col, xl * 2 + core, xr * 2 + core, xo * 2 + core, xo * 2 + core]
    begin = [0, 0, 0, 0, 128]
    length = [KS, KS, KS, 128, 128]

    def wtile(k, g):
        return wfull.at[pl.ds(pl.multiple_of(same[k] * KS + begin[k], 128), length[k]), pl.ds(pl.multiple_of(g * GRP, GRP), GRP)]

    def other(k, g):
        return wfull.at[pl.ds(pl.multiple_of((same[k] + 1 - 2 * core) * KS + begin[k], 128), length[k]), pl.ds(pl.multiple_of(g * GRP, GRP), GRP)]

    def push(ref, ss, rs, peer):
        return pltpu.make_async_remote_copy(src_ref=ref, dst_ref=ref, send_sem=ss, recv_sem=rs, device_id=peer, device_id_type=MESH)

    xg = (y, yo)
    yg = (yu, yd)

    def along_x(t, k):
        piece = (0, 0, 3, 4)[k]
        who = (None, None, xl * 2 + core, xr * 2 + core)[k]
        ref = wtile(0, xg[t])
        if k >= 2:
            ref = wfull.at[pl.ds(pl.multiple_of(who * KS + begin[piece], 128), 128), pl.ds(pl.multiple_of(xg[t] * GRP, GRP), GRP)]
        return push(ref, pin_s.at[t, k], pin_r.at[t, k], {"col": (right, left, right, left)[k]})

    def x_arrived(t, k):
        along_x(t, k).wait_recv()

    def to_mate(t, k):
        return push(wtile(k, (*xg, *yg)[t]), ymt_s.at[t, k], ymt_r.at[t, k], {"col": mate})

    def from_mate(t, k):
        push(other(k, (*xg, *yg)[t]), ymt_s.at[t, k], ymt_r.at[t, k], {"col": mate}).wait_recv()

    def along_y(d, k):
        return push(wtile(k, y), yin_s.at[d, k], yin_r.at[d, k], {"row": at(0, (yu, yd)[d])})

    def y_arrived(d, k):
        push(wtile(k, (yd, yu)[d]), yin_s.at[d, k], yin_r.at[d, k], {"row": at(0, (yu, yd)[d])}).wait_recv()

    def piece_in(t, k):
        to_mate(t, k).start()
        if t == 0 and k > 0:
            along_y(0, k).start()
            along_y(1, k).start()

    along_x(0, 0).start()
    along_x(0, 1).start()
    piece_in(0, 0)
    along_x(1, 0).start()
    along_x(1, 1).start()
    piece_in(1, 0)
    to_mate(2, 0).start()
    to_mate(3, 0).start()

    def tell(i, peers):
        for peer in peers:
            pl.semaphore_signal(hops.at[i], inc=1, device_id={"row": peer}, device_id_type=MESH)

    tell(0, (at(1, y), at(NZ - 1, y), at(0, yu), at(0, yd)))

    rid = lax.broadcasted_iota(jnp.int32, (FW, FW), 1)
    fid = lax.broadcasted_iota(jnp.int32, (FW, FW), 0)
    inner = lax.rem(rid, 256)
    slot = (inner // 16) * 4 + lax.rem(inner, 4)
    upper = jnp.where(slot == 0, 64, GRP - slot)
    want = lax.rem(inner // 4, 4) * GRP + jnp.where(rid < 256, slot, upper)
    perm = jnp.where(fid == want, 1.0, 0.0).astype(BF)
    loads[1].wait()
    blk[...] = jnp.dot(pblk[...], perm, preferred_element_type=F32).astype(BF)

    pl.semaphore_wait(hops.at[0], 4)
    tell(1, (at(2, y), at(NZ - 2, y)))

    for i in (3, 4, 5, 6):
        loads[i].wait()
    lane = lax.rem(lax.broadcasted_iota(jnp.int32, (2 * LOC, 4 * LOC), 1), 4)
    sub = lax.rem(lax.broadcasted_iota(jnp.int32, (256, 256), 0), 4)
    for s in range(4):
        m1[s] = first[...] * jnp.where(lane == s, 1.0, 0.0).astype(BF)
        l3[s] = last[...] * jnp.where(sub == s, 1.0, 0.0).astype(BF)

    pl.semaphore_wait(hops.at[1], 2)
    tell(2, (at(4, y), at(NZ - 4, y)))

    for t in range(2):
        x_arrived(t, 0)
        along_x(t, 2).start()
        piece_in(t, 1)
        x_arrived(t, 1)
        along_x(t, 3).start()
        piece_in(t, 2)

    pl.semaphore_wait(hops.at[2], 2)
    tell(3, (at(0, yu), at(0, yd), at(0, yo)))

    for k in (3, 4):
        x_arrived(0, k - 1)
        piece_in(0, k)
    for k in (3, 4):
        x_arrived(1, k - 1)
        piece_in(1, k)
    for d in range(2):
        for k in (1, 2):
            y_arrived(d, k)
            to_mate(3 - d, k).start()
    loads[2].wait()

    pl.semaphore_wait(hops.at[3], 3)

    half = pl.ds(pl.multiple_of(core * 16, 16), 16)
    quarter = pl.ds(pl.multiple_of(x * GRP, GRP), GRP)
    own = pltpu.make_async_copy(blk.at[half, quarter], pgx.at[row], ld.at[7])
    own.start()

    def far(i):
        step = (i + 1) // 2
        return lax.rem(8 + step * (1 - 2 * lax.rem(i, 2)) + NZ, NZ)

    def pz_send(i, c):
        pltpu.make_async_remote_copy(src_ref=blk.at[half, quarter], dst_ref=pgx.at[row], send_sem=pz_s, recv_sem=pz_r, device_id={"row": at(far(i), y)}, device_id_type=MESH).start()
        return c

    lax.fori_loop(0, NZ - 1, pz_send, 0)
    own.wait()

    order = (y, yo, yu, yd)
    for t in range(GROUPS):
        g = order[t]
        if t == 2:
            for d in range(2):
                for k in (3, 4):
                    y_arrived(d, k)
                    to_mate(3 - d, k).start()
        for k in range(5):
            from_mate(t, k)
        w = wfull[:, pl.ds(pl.multiple_of(g * GRP, GRP), GRP)]
        mapped = jnp.dot(tok[...], w, preferred_element_type=F32).astype(BF)
        zero = jnp.zeros((64, GRP), BF)
        parts = []
        for m in range(3):
            piece = mapped[64 * m : 64 * m + 64]
            parts.append(jnp.concatenate([piece, zero], 1))
            parts.append(jnp.concatenate([zero, piece], 1))
        spread = bdot(chan[...], jnp.concatenate(parts, 0))
        for m in range(3):
            snd[t, :, m] = spread[:, GRP * m : GRP * m + GRP].reshape(NZ, 4, GRP).astype(BF)

        def a1_send(i, c, t=t, g=g):
            to = lax.rem(z + far(i), NZ)
            pltpu.make_async_remote_copy(src_ref=snd.at[t, to], dst_ref=dat.at[row], send_sem=a1_s.at[t], recv_sem=a1_r, device_id={"row": to * NY + g}, device_id_type=MESH).start()
            return c

        lax.fori_loop(0, NZ - 1 if t == 0 else NZ, a1_send, 0)
        if t == 0:
            pltpu.make_async_copy(snd.at[0, z], dat.at[row], a1_r).start()

    pltpu.make_async_copy(pgx.at[pl.ds(0, NZ - 1)], pgx.at[pl.ds(0, NZ - 1)], pz_r).wait()
    for o in range(1, NY):

        def py_send(k, c, o=o):
            pltpu.make_async_remote_copy(src_ref=pgx.at[k * NY + y], dst_ref=pgx.at[k * NY + y], send_sem=py_s.at[o - 1], recv_sem=py_r, device_id={"row": at(0, lax.rem(y + o, NY))}, device_id_type=MESH).start()
            return c

        lax.fori_loop(0, NZ, py_send, 0)

    pltpu.make_async_copy(pgx.at[pl.ds(0, 3 * NZ)], pgx.at[pl.ds(0, 3 * NZ)], py_r).wait()

    def ptile(c, lo=0, n=ROWS):
        return pt.at[pl.ds(lo, n), pl.ds(pl.multiple_of(lax.rem(c, 2) * 16, 16), 16), pl.ds(pl.multiple_of((c // 2) * GRP, GRP), GRP)]

    mine = pltpu.make_async_copy(pgx, ptile(col), ld.at[8])
    mine.start()
    mine.wait()

    def px(k):
        who = (col, col, col, xl * 2 + core, xr * 2 + core, xl * 2 + core, xr * 2 + core, xo * 2 + core, xo * 2 + core)[k]
        lo = (0, 0, 0, 0, 32, 0, 0, 0, 32)[k]
        n = (64, 64, 64, 32, 32, 64, 64, 32, 32)[k]
        peer = (right, left, mate, right, left, mate, mate, mate, mate)[k]
        return push(ptile(who, lo, n), px_s.at[k], px_r.at[k], {"col": peer})

    def px_arrived(k):
        n = (64, 64, 64, 32, 32, 64, 64, 32, 32)[k]
        push(ptile(col, 0, n), px_s.at[k], px_r.at[k], {"col": mate}).wait_recv()

    for k in range(3):
        px(k).start()

    pltpu.make_async_copy(dat, dat, a1_r).wait()
    data = dat[...].reshape(4 * LOC, GRP)
    cc, sn = twist[0], twist[1]
    first_slot = z == 0
    lanes = lax.broadcasted_iota(jnp.int32, (1, GRP), 1) < 64
    sgn = jnp.where(lanes, 1.0, -1.0)
    zero_b = jnp.where(lanes, 1.0, 0.0)
    spec = jnp.where(first_slot, 1.0, 0.0)
    outs = [None] * 3
    for s in range(4):
        got = jnp.dot(m1[s], data, preferred_element_type=F32)
        re, im = got[:LOC], got[LOC:]
        tre = re * cc - im * sn
        tim = re * sn + im * cc
        if s == 0:
            lo_mask = zero_b * spec + sgn * (1.0 - spec)
            up_keep, up_turn = 1.0 - spec, zero_b * spec
            lo_re, lo_im = tre * lo_mask, tim * lo_mask
            up_re = tre * up_keep + pltpu.roll(tre, 64, 1) * up_turn
            up_im = tim * up_keep + pltpu.roll(tim, 64, 1) * up_turn
        else:
            lo_re, lo_im, up_re, up_im = tre * sgn, tim * sgn, tre, tim
        lo = jnp.concatenate([lo_re, lo_im], 1).astype(BF)
        up = jnp.concatenate([up_re, up_im], 1).astype(BF)
        for m in range(3):
            rhs = jnp.concatenate([lo[64 * m : 64 * m + 64], up[64 * m : 64 * m + 64]], 0)
            term = bdot(l3[s], rhs)
            outs[m] = term if outs[m] is None else outs[m] + term
    for m in range(3):
        snd2[:, m] = outs[m].reshape(ROWS, 4, GRP).astype(BF)

    pltpu.make_async_copy(snd2.at[row], dat2.at[row], a2_r).start()

    def a2_send(i, c):
        to = at(far(i // NY), lax.rem(y + lax.rem(i + 1, NY), NY))
        pltpu.make_async_remote_copy(src_ref=snd2.at[to], dst_ref=dat2.at[row], send_sem=a2_s, recv_sem=a2_r, device_id={"row": to}, device_id_type=MESH).start()
        return c

    lax.fori_loop(0, ROWS - 1, a2_send, 0)

    px_arrived(0)
    px(3).start()
    px(5).start()
    px_arrived(1)
    px(4).start()
    px(6).start()
    px_arrived(3)
    px(7).start()
    px_arrived(4)
    px(8).start()
    for k in (2, 5, 6, 7, 8):
        px_arrived(k)

    pltpu.make_async_copy(dat2, dat2, a2_r).wait()
    sides = []
    for m in range(3):
        t = dat2[:, m].reshape(256, GRP).T
        sides.append(jnp.concatenate([t[:64], t[64:]], 1))
    lhs = jnp.concatenate(sides, 0)
    for n in range(8):
        out_ref[0, :, 256 * n : 256 * n + 256] = bdot(lhs, pt[8 * n : 8 * n + 8].reshape(256, FW)).astype(BF)

    for t in range(2):
        for k in range(4):
            along_x(t, k).wait_send()
    for k in range(5):
        for d in range(2 if k else 0):
            along_y(d, k).wait_send()
        for t in range(4):
            to_mate(t, k).wait_send()
    for t in range(GROUPS):
        n = NZ - 1 if t == 0 else NZ
        pltpu.make_async_copy(snd.at[t, pl.ds(0, n)], snd.at[t, pl.ds(0, n)], a1_s.at[t]).wait()
    for k in range(9):
        px(k).wait_send()
    pltpu.make_async_copy(pgx.at[pl.ds(0, NZ - 1)], pgx.at[pl.ds(0, NZ - 1)], pz_s).wait()
    for o in range(3):
        pltpu.make_async_copy(pgx.at[pl.ds(0, NZ)], pgx.at[pl.ds(0, NZ)], py_s.at[o]).wait()
    pltpu.make_async_copy(snd2.at[pl.ds(0, ROWS - 1)], snd2.at[pl.ds(0, ROWS - 1)], a2_s).wait()


def shards(tokens, proj_in, proj_out):
    chan, first, twist, last = tables()
    anyspec = pl.BlockSpec(memory_space=pl.ANY)
    dma = pltpu.SemaphoreType.DMA
    return pl.pallas_call(
        kernel,
        out_shape=jax.ShapeDtypeStruct((1, LOC, D), BF),
        in_specs=[anyspec] * 7,
        out_specs=pl.BlockSpec(memory_space=pltpu.VMEM),
        scratch_shapes=[
            pltpu.VMEM((LOC, D), BF),
            pltpu.VMEM((D, FW), BF),
            pltpu.VMEM((32, FW), BF),
            pltpu.VMEM((64, 256), BF),
            pltpu.VMEM((2 * LOC, 4 * LOC), BF),
            pltpu.VMEM((2, LOC, GRP), F32),
            pltpu.VMEM((256, 256), BF),
            pltpu.VMEM((4, 2 * LOC, 4 * LOC), BF),
            pltpu.VMEM((4, 256, 256), BF),
            pltpu.VMEM((32, FW), BF),
            pltpu.VMEM((ROWS, 32, FW), BF),
            pltpu.VMEM((GROUPS, NZ, 3, 4, GRP), BF),
            pltpu.VMEM((ROWS, 3, 4, GRP), BF),
            pltpu.VMEM((ROWS, 3, 4, GRP), BF),
            pltpu.VMEM((ROWS, 3, 4, GRP), BF),
            pltpu.VMEM((ROWS, 16, GRP), BF),
            dma((9,)),
            pltpu.SemaphoreType.REGULAR((4,)),
            dma((2, 4)),
            dma((2, 4)),
            dma((2, 5)),
            dma((2, 5)),
            dma((4, 5)),
            dma((4, 5)),
            dma((GROUPS,)),
            dma,
            dma,
            dma,
            dma,
            dma,
            dma((3,)),
            dma,
            dma((9,)),
            dma((9,)),
        ],
        compiler_params=pltpu.CompilerParams(collective_id=0, has_side_effects=True),
    )(
        tokens,
        proj_in,
        proj_out.T,
        jnp.asarray(chan, BF),
        jnp.asarray(first, BF),
        jnp.asarray(twist, F32),
        jnp.asarray(last, BF),
    )


def solution(mesh):
    return jax.shard_map(
        shards,
        mesh=mesh,
        in_specs=(P("col", "row", None), P("col", None), P(None, "row")),
        out_specs=P("col", "row", None),
        check_vma=False,
    )
```

```python
import math

import jax
import jax.numpy as jnp
import numpy as np
from jax import lax
from jax.experimental import pallas as pl
from jax.experimental.pallas import tpu as pltpu
from jax.sharding import PartitionSpec as P

MESH = pl.DeviceIdType.MESH
GRP = 128
GROUPS = 4
NZ, NY, NX = 16, 4, 4
ROWS = NZ * NY
LOC = 192
LEN = ROWS * LOC
D = 2048
KS = 256
FW = GROUPS * GRP
F32 = jnp.float32
BF = jnp.bfloat16


def tables():
    s = np.arange(64)[:, None]
    f = np.arange(GRP)[None, :]
    ang = 2 * np.pi * ((s * f) % GRP) / GRP
    part_a = np.cos(ang)
    part_b = np.sin(ang)
    part_b[0] = np.cos(np.pi * np.arange(GRP))
    chan = np.concatenate([part_a, part_b], 1)
    q = np.arange(LOC)[:, None]
    p1 = np.arange(LOC)[None, :]
    ang = 2 * np.pi * ((q * p1) % LOC) / LOC
    first = np.repeat(np.concatenate([np.cos(ang), np.sin(ang)], 0), 4, axis=1)
    q2 = np.arange(64)[None, :]
    ang = 2 * np.pi * ((q * q2) % LEN) / LEN
    scale = 1.0 / math.sqrt(GRP * LEN)
    twist = np.stack([np.tile(np.cos(ang), (1, 2)), np.tile(np.sin(ang), (1, 2))]) * scale
    r = np.arange(64)[:, None]
    ang = 2 * np.pi * ((r * q2) % 64) / 64
    c, n = np.cos(ang), np.sin(ang)
    last = np.repeat(np.concatenate([c, n, -n, c], 1), 4, axis=0)
    return chan, first, twist, last


def bdot(a, b):
    return lax.dot_general(a, b, (((1,), (1,)), ((), ())), preferred_element_type=F32)


def kernel(tok_hbm, win_hbm, pout_hbm, chan_hbm, first_hbm, twist_hbm, last_hbm, lhs_ref, pt, tok, wfull, pblk, chan, first, twist, last, m1, l3, blk, snd, dat, snd2, dat2, ld, hops, pin_s, pin_r, yin_s, yin_r, ymt_s, ymt_r, a1_s, a1_r, a2_s, a2_r, pz_s, pz_r, py_s, py_r, px_s, px_r):
    row = lax.axis_index("row")
    col = lax.axis_index("col")
    z, y = row // NY, lax.rem(row, NY)
    x, core = col // 2, lax.rem(col, 2)
    xr = lax.rem(x + 1, NX)
    xl = lax.rem(x + NX - 1, NX)
    xo = lax.rem(x + 2, NX)
    right, left, mate = xr * 2 + core, xl * 2 + core, x * 2 + (1 - core)
    yu, yd, yo = lax.rem(y + 1, NY), lax.rem(y + NY - 1, NY), lax.rem(y + 2, NY)

    def at(dz, yy):
        return lax.rem(z + dz, NZ) * NY + yy

    bar = pltpu.get_barrier_semaphore()
    for peer in (right, left, xo * 2 + core, mate):
        pl.semaphore_signal(bar, inc=1, device_id={"col": peer}, device_id_type=MESH)
    for peer in (at(0, yu), at(0, yd), at(1, y), at(NZ - 1, y)):
        pl.semaphore_signal(bar, inc=1, device_id={"row": peer}, device_id_type=MESH)

    loads = [
        pltpu.make_async_copy(win_hbm, wfull.at[pl.ds(pl.multiple_of(col * KS, KS), KS), :], ld.at[0]),
        pltpu.make_async_copy(pout_hbm, pblk, ld.at[1]),
        pltpu.make_async_copy(tok_hbm.at[0], tok, ld.at[2]),
        pltpu.make_async_copy(chan_hbm, chan, ld.at[3]),
        pltpu.make_async_copy(first_hbm, first, ld.at[4]),
        pltpu.make_async_copy(last_hbm, last, ld.at[5]),
        pltpu.make_async_copy(twist_hbm, twist, ld.at[6]),
    ]
    for c in loads:
        c.start()
    pl.semaphore_wait(bar, 8)

    def tell(i, peers):
        for peer in peers:
            pl.semaphore_signal(hops.at[i], inc=1, device_id={"row": peer}, device_id_type=MESH)

    tell(0, (at(1, y), at(NZ - 1, y), at(0, yu), at(0, yd)))
    loads[0].wait()

    same = [col, xl * 2 + core, xr * 2 + core, xo * 2 + core]

    def tile(c, g):
        return wfull.at[pl.ds(pl.multiple_of(c * KS, KS), KS), pl.ds(pl.multiple_of(g * GRP, GRP), GRP)]

    def push(ref, ss, rs, peer):
        return pltpu.make_async_remote_copy(src_ref=ref, dst_ref=ref, send_sem=ss, recv_sem=rs, device_id=peer, device_id_type=MESH)

    order = (y, yo, yu, yd)

    def along_x(t, k):
        return push(tile(col, order[t]), pin_s.at[t, k], pin_r.at[t, k], {"col": (right, left, xo * 2 + core)[k]})

    def to_mate(t, k):
        return push(tile(same[k], order[t]), ymt_s.at[t, k], ymt_r.at[t, k], {"col": mate})

    def from_mate(t, k):
        push(tile(same[k] + 1 - 2 * core, order[t]), ymt_s.at[t, k], ymt_r.at[t, k], {"col": mate}).wait_recv()

    def along_y(d, k):
        return push(tile(same[k], y), yin_s.at[d, k - 1], yin_r.at[d, k - 1], {"row": at(0, (yu, yd)[d])})

    def y_passed(d, k):
        push(tile(same[k], (yd, yu)[d]), yin_s.at[d, k - 1], yin_r.at[d, k - 1], {"row": at(0, (yu, yd)[d])}).wait_recv()
        to_mate(3 - d, k).start()

    def x_passed(t, k):
        along_x(t, k).wait_recv()
        to_mate(t, k + 1).start()
        if t == 0:
            along_y(0, k + 1).start()
            along_y(1, k + 1).start()

    for k in range(3):
        along_x(0, k).start()
    to_mate(0, 0).start()

    rid = lax.broadcasted_iota(jnp.int32, (FW, FW), 1)
    fid = lax.broadcasted_iota(jnp.int32, (FW, FW), 0)
    inner = lax.rem(rid, 256)
    slot = (inner // 16) * 4 + lax.rem(inner, 4)
    upper = jnp.where(slot == 0, 64, GRP - slot)
    want = lax.rem(inner // 4, 4) * GRP + jnp.where(rid < 256, slot, upper)
    perm = jnp.where(fid == want, 1.0, 0.0).astype(BF)
    loads[1].wait()
    blk[...] = jnp.dot(pblk[...], perm, preferred_element_type=F32).astype(BF)

    half = pl.ds(pl.multiple_of(core * 16, 16), 16)
    quarter = pl.ds(pl.multiple_of(x * GRP, GRP), GRP)

    def mine(yy, c=None):
        c = col if c is None else c
        return pt.at[yy, :, pl.ds(pl.multiple_of(lax.rem(c, 2) * 16, 16), 16), pl.ds(pl.multiple_of((c // 2) * GRP, GRP), GRP)]

    own = pltpu.make_async_copy(blk.at[half, quarter], pt.at[y, z, half, quarter], ld.at[7])
    own.start()

    def pz_send(dz):
        pltpu.make_async_remote_copy(src_ref=blk.at[half, quarter], dst_ref=pt.at[y, z, half, quarter], send_sem=pz_s, recv_sem=pz_r, device_id={"row": at(dz, y)}, device_id_type=MESH).start()

    pl.semaphore_wait(hops.at[0], 4)
    tell(1, (at(2, y), at(NZ - 2, y)))
    for dz in (1, 15, 2, 14):
        pz_send(dz)

    for i in (3, 4, 5, 6):
        loads[i].wait()
    lane = lax.rem(lax.broadcasted_iota(jnp.int32, (2 * LOC, 4 * LOC), 1), 4)
    sub = lax.rem(lax.broadcasted_iota(jnp.int32, (256, 256), 0), 4)
    for s in range(4):
        m1[s] = first[...] * jnp.where(lane == s, 1.0, 0.0).astype(BF)
        l3[s] = last[...] * jnp.where(sub == s, 1.0, 0.0).astype(BF)

    pl.semaphore_wait(hops.at[1], 2)
    tell(2, (at(4, y), at(NZ - 4, y)))
    for dz in (3, 13, 4, 12):
        pz_send(dz)

    for k in range(3):
        x_passed(0, k)
        if k == 1:
            for j in range(3):
                along_x(1, j).start()
            for t in range(1, 4):
                to_mate(t, 0).start()

    pl.semaphore_wait(hops.at[2], 2)
    tell(3, (at(0, yu), at(0, yd), at(0, yo)))
    for dz in (8, 7, 9, 6, 10, 5, 11):
        pz_send(dz)
    own.wait()
    loads[2].wait()

    def far(i):
        step = (i + 1) // 2
        return lax.rem(8 + step * (1 - 2 * lax.rem(i, 2)) + NZ, NZ)

    peers_y = (yu, yd, yo)

    def py(o):
        return push(mine(y), py_s.at[o], py_r.at[o], {"row": at(0, peers_y[o])})

    def py_passed(o):
        push(mine((yd, yu, yo)[o]), py_s.at[o], py_r.at[o], {"row": row}).wait_recv()
        px_out(o + 1)

    whose = (y, yd, yu, yo)

    def px(u, k):
        c = (col, col, col, col, xl * 2 + core, xr * 2 + core, xo * 2 + core)[k]
        peer = (right, left, xo * 2 + core, mate, mate, mate, mate)[k]
        return push(mine(whose[u], c), px_s.at[u, k], px_r.at[u, k], {"col": peer})

    def px_out(u):
        for k in range(4):
            px(u, k).start()

    def px_passed(u):
        for k in range(3):
            px(u, k).wait_recv()
            px(u, k + 4).start()

    for t in range(GROUPS):
        g = order[t]
        if t == 1:
            pl.semaphore_wait(hops.at[3], 3)
            for k in range(3):
                x_passed(1, k)
            for k in (1, 2):
                for d in range(2):
                    y_passed(d, k)
        if t == 2:
            for d in range(2):
                y_passed(d, 3)
            part = pt.at[y, pl.ds(0, NZ - 1), half, quarter]
            pltpu.make_async_copy(part, part, pz_r).wait()
            for o in range(3):
                py(o).start()
            px_out(0)
        for k in range(4):
            from_mate(t, k)
        w = wfull[:, pl.ds(pl.multiple_of(g * GRP, GRP), GRP)]
        mapped = jnp.dot(tok[...], w, preferred_element_type=F32).astype(BF)
        zero = jnp.zeros((64, GRP), BF)
        parts = []
        for m in range(3):
            piece = mapped[64 * m : 64 * m + 64]
            parts.append(jnp.concatenate([piece, zero], 1))
            parts.append(jnp.concatenate([zero, piece], 1))
        spread = bdot(chan[...], jnp.concatenate(parts, 0))
        for m in range(3):
            snd[t, :, m] = spread[:, GRP * m : GRP * m + GRP].reshape(NZ, 4, GRP).astype(BF)

        def a1_send(i, c, t=t, g=g):
            to = lax.rem(z + far(i), NZ)
            pltpu.make_async_remote_copy(src_ref=snd.at[t, to], dst_ref=dat.at[row], send_sem=a1_s.at[t], recv_sem=a1_r, device_id={"row": to * NY + g}, device_id_type=MESH).start()
            return c

        lax.fori_loop(0, NZ - 1 if t == 0 else NZ, a1_send, 0)
        if t == 0:
            pltpu.make_async_copy(snd.at[0, z], dat.at[row], a1_r).start()

    for t in range(2):
        for k in range(3):
            along_x(t, k).wait_send()
    for k in range(4):
        for t in range(4):
            to_mate(t, k).wait_send()
        if k:
            for d in range(2):
                along_y(d, k).wait_send()

    for o in range(3):
        py_passed(o)

    pltpu.make_async_copy(dat, dat, a1_r).wait()
    data = dat[...].reshape(4 * LOC, GRP)
    cc, sn = twist[0], twist[1]
    first_slot = z == 0
    lanes = lax.broadcasted_iota(jnp.int32, (1, GRP), 1) < 64
    sgn = jnp.where(lanes, 1.0, -1.0)
    zero_b = jnp.where(lanes, 1.0, 0.0)
    spec = jnp.where(first_slot, 1.0, 0.0)
    outs = [None] * 3
    for s in range(4):
        got = jnp.dot(m1[s], data, preferred_element_type=F32)
        re, im = got[:LOC], got[LOC:]
        tre = re * cc - im * sn
        tim = re * sn + im * cc
        if s == 0:
            lo_mask = zero_b * spec + sgn * (1.0 - spec)
            up_keep, up_turn = 1.0 - spec, zero_b * spec
            lo_re, lo_im = tre * lo_mask, tim * lo_mask
            up_re = tre * up_keep + pltpu.roll(tre, 64, 1) * up_turn
            up_im = tim * up_keep + pltpu.roll(tim, 64, 1) * up_turn
        else:
            lo_re, lo_im, up_re, up_im = tre * sgn, tim * sgn, tre, tim
        lo = jnp.concatenate([lo_re, lo_im], 1).astype(BF)
        up = jnp.concatenate([up_re, up_im], 1).astype(BF)
        for m in range(3):
            rhs = jnp.concatenate([lo[64 * m : 64 * m + 64], up[64 * m : 64 * m + 64]], 0)
            term = bdot(l3[s], rhs)
            outs[m] = term if outs[m] is None else outs[m] + term
    for m in range(3):
        snd2[:, m] = outs[m].reshape(ROWS, 4, GRP).astype(BF)

    pltpu.make_async_copy(snd2.at[row], dat2.at[row], a2_r).start()

    def a2_send(i, c):
        to = at(far(i // NY), lax.rem(y + lax.rem(i + 1, NY), NY))
        pltpu.make_async_remote_copy(src_ref=snd2.at[to], dst_ref=dat2.at[row], send_sem=a2_s, recv_sem=a2_r, device_id={"row": to}, device_id_type=MESH).start()
        return c

    lax.fori_loop(0, ROWS - 1, a2_send, 0)

    for u in range(4):
        px_passed(u)
    for u in range(4):
        for k in range(3, 7):
            px(u, k).wait_recv()

    for t in range(GROUPS):
        n = NZ - 1 if t == 0 else NZ
        pltpu.make_async_copy(snd.at[t, pl.ds(0, n)], snd.at[t, pl.ds(0, n)], a1_s.at[t]).wait()
    for u in range(4):
        for k in range(7):
            px(u, k).wait_send()
    pltpu.make_async_copy(part, part, pz_s).wait()
    for o in range(3):
        py(o).wait_send()
    pltpu.make_async_copy(snd2.at[pl.ds(0, ROWS - 1)], snd2.at[pl.ds(0, ROWS - 1)], a2_s).wait()

    pltpu.make_async_copy(dat2, dat2, a2_r).wait()
    sides = []
    for m in range(3):
        t = dat2[:, m].reshape(256, GRP).T
        sides.append(jnp.concatenate([t[:64], t[64:]], 1))
    lhs = jnp.concatenate(sides, 0)
    lhs_ref[...] = lhs


def product(lhs_ref, pt_ref, out_hbm, out, sem):
    wide = D // 8
    copies = []
    for n in range(8):
        cols = pl.ds(wide * n, wide)
        rhs = jnp.concatenate([pt_ref[yy, zz] for zz in (2 * n, 2 * n + 1) for yy in range(NY)], 0)
        out[:, cols] = bdot(lhs_ref[...], rhs).astype(BF)
        copies.append(pltpu.make_async_copy(out.at[:, cols], out_hbm.at[0, :, cols], sem.at[n]))
        copies[-1].start()
    for c in copies:
        c.wait()


def shards(tokens, proj_in, proj_out):
    chan, first, twist, last = tables()
    anyspec = pl.BlockSpec(memory_space=pltpu.HBM)
    dma = pltpu.SemaphoreType.DMA
    lhs, pt = pl.pallas_call(
        kernel,
        out_shape=(jax.ShapeDtypeStruct((LOC, FW), BF), jax.ShapeDtypeStruct((NY, NZ, 32, FW), BF)),
        in_specs=[anyspec] * 7,
        out_specs=(pl.BlockSpec(memory_space=pltpu.VMEM), pl.BlockSpec(memory_space=pltpu.VMEM)),
        scratch_shapes=[
            pltpu.VMEM((LOC, D), BF),
            pltpu.VMEM((D, FW), BF),
            pltpu.VMEM((32, FW), BF),
            pltpu.VMEM((64, 256), BF),
            pltpu.VMEM((2 * LOC, 4 * LOC), BF),
            pltpu.VMEM((2, LOC, GRP), F32),
            pltpu.VMEM((256, 256), BF),
            pltpu.VMEM((4, 2 * LOC, 4 * LOC), BF),
            pltpu.VMEM((4, 256, 256), BF),
            pltpu.VMEM((32, FW), BF),
            pltpu.VMEM((GROUPS, NZ, 3, 4, GRP), BF),
            pltpu.VMEM((ROWS, 3, 4, GRP), BF),
            pltpu.VMEM((ROWS, 3, 4, GRP), BF),
            pltpu.VMEM((ROWS, 3, 4, GRP), BF),
            dma((9,)),
            pltpu.SemaphoreType.REGULAR((4,)),
            dma((2, 3)),
            dma((2, 3)),
            dma((2, 3)),
            dma((2, 3)),
            dma((4, 4)),
            dma((4, 4)),
            dma((GROUPS,)),
            dma,
            dma,
            dma,
            dma,
            dma,
            dma((3,)),
            dma((3,)),
            dma((4, 7)),
            dma((4, 7)),
        ],
        compiler_params=pltpu.CompilerParams(collective_id=0, has_side_effects=True, vmem_limit_bytes=24 << 20),
    )(
        *(
            pltpu.with_memory_space_constraint(a, pltpu.HBM)
            for a in (tokens, proj_in, proj_out.T, jnp.asarray(chan, BF), jnp.asarray(first, BF), jnp.asarray(twist, F32), jnp.asarray(last, BF))
        )
    )
    return pl.pallas_call(
        product,
        out_shape=jax.ShapeDtypeStruct((1, LOC, D), BF),
        in_specs=[pl.BlockSpec(memory_space=pltpu.VMEM)] * 2,
        out_specs=pl.BlockSpec(memory_space=pl.ANY),
        scratch_shapes=[pltpu.VMEM((LOC, D), BF), dma((8,))],
        compiler_params=pltpu.CompilerParams(vmem_limit_bytes=24 << 20),
    )(lhs, pt)


def solution(mesh):
    return jax.shard_map(
        shards,
        mesh=mesh,
        in_specs=(P("col", "row", None), P("col", None), P(None, "row")),
        out_specs=P("col", "row", None),
        check_vma=False,
    )
```

```python
import math

import jax
import jax.numpy as jnp
import numpy as np
from jax import lax
from jax.experimental import pallas as pl
from jax.experimental.pallas import tpu as pltpu
from jax.sharding import PartitionSpec as P

MESH = pl.DeviceIdType.MESH
GRP = 128
GROUPS = 4
NZ, NY, NX = 16, 4, 4
ROWS = NZ * NY
LOC = 192
LEN = ROWS * LOC
D = 2048
KS = 256
FW = GROUPS * GRP
F32 = jnp.float32
BF = jnp.bfloat16


def tables():
    s = np.arange(64)[:, None]
    f = np.arange(GRP)[None, :]
    ang = 2 * np.pi * ((s * f) % GRP) / GRP
    part_a = np.cos(ang)
    part_b = np.sin(ang)
    part_b[0] = np.cos(np.pi * np.arange(GRP))
    chan = np.concatenate([part_a, part_b], 1)
    q = np.arange(LOC)[:, None]
    p1 = np.arange(LOC)[None, :]
    ang = 2 * np.pi * ((q * p1) % LOC) / LOC
    first = np.repeat(np.concatenate([np.cos(ang), np.sin(ang)], 0), 4, axis=1)
    q2 = np.arange(64)[None, :]
    ang = 2 * np.pi * ((q * q2) % LEN) / LEN
    scale = 1.0 / math.sqrt(GRP * LEN)
    twist = np.stack([np.tile(np.cos(ang), (1, 2)), np.tile(np.sin(ang), (1, 2))]) * scale
    r = np.arange(64)[:, None]
    ang = 2 * np.pi * ((r * q2) % 64) / 64
    c, n = np.cos(ang), np.sin(ang)
    last = np.repeat(np.concatenate([c, n, -n, c], 1), 4, axis=0)
    return chan, first, twist, last


def bdot(a, b):
    return lax.dot_general(a, b, (((1,), (1,)), ((), ())), preferred_element_type=F32)


def kernel(tok_hbm, win_hbm, pout_hbm, chan_hbm, first_hbm, twist_hbm, last_hbm, lhs_ref, pt, tok, wfull, pblk, chan, first, twist, last, m1, l3, blk, snd, dat, snd2, dat2, ld, hops, w_s, pin_r, yin_r, ymt_r, a1_s, a1_r, a2_s, a2_r, pz_s, pz_r, p_s, py_r, px_r):
    row = lax.axis_index("row")
    col = lax.axis_index("col")
    z, y = row // NY, lax.rem(row, NY)
    x, core = col // 2, lax.rem(col, 2)
    xr = lax.rem(x + 1, NX)
    xl = lax.rem(x + NX - 1, NX)
    xo = lax.rem(x + 2, NX)
    right, left, mate = xr * 2 + core, xl * 2 + core, x * 2 + (1 - core)
    yu, yd, yo = lax.rem(y + 1, NY), lax.rem(y + NY - 1, NY), lax.rem(y + 2, NY)

    def at(dz, yy):
        return lax.rem(z + dz, NZ) * NY + yy

    bar = pltpu.get_barrier_semaphore()
    for peer in (right, left, xo * 2 + core, mate):
        pl.semaphore_signal(bar, inc=1, device_id={"col": peer}, device_id_type=MESH)
    for peer in (at(0, yu), at(0, yd), at(1, y), at(NZ - 1, y)):
        pl.semaphore_signal(bar, inc=1, device_id={"row": peer}, device_id_type=MESH)

    loads = [
        pltpu.make_async_copy(win_hbm, wfull.at[pl.ds(pl.multiple_of(col * KS, KS), KS), :], ld.at[0]),
        pltpu.make_async_copy(pout_hbm, pblk, ld.at[1]),
        pltpu.make_async_copy(tok_hbm.at[0], tok, ld.at[2]),
        pltpu.make_async_copy(chan_hbm, chan, ld.at[3]),
        pltpu.make_async_copy(first_hbm, first, ld.at[3]),
        pltpu.make_async_copy(last_hbm, last, ld.at[3]),
        pltpu.make_async_copy(twist_hbm, twist, ld.at[3]),
    ]
    for c in loads:
        c.start()
    pl.semaphore_wait(bar, 8)

    def tell(i, peers):
        for peer in peers:
            pl.semaphore_signal(hops.at[i], inc=1, device_id={"row": peer}, device_id_type=MESH)

    tell(0, (at(1, y), at(NZ - 1, y), at(0, yu), at(0, yd)))
    loads[0].wait()

    same = [col, xl * 2 + core, xr * 2 + core, xo * 2 + core]

    def tile(c, g):
        return wfull.at[pl.ds(pl.multiple_of(c * KS, KS), KS), pl.ds(pl.multiple_of(g * GRP, GRP), GRP)]

    def arrived(rows, sem):
        pltpu.make_async_copy(wfull.at[pl.ds(0, rows)], wfull.at[pl.ds(0, rows)], sem).wait()

    def push(ref, ss, rs, peer):
        return pltpu.make_async_remote_copy(src_ref=ref, dst_ref=ref, send_sem=ss, recv_sem=rs, device_id=peer, device_id_type=MESH)

    order = (y, yo, yu, yd)

    def along_x(t, k):
        return push(tile(col, order[t]), w_s, pin_r.at[k if t == 0 else 3], {"col": (right, left, xo * 2 + core)[k]})

    def to_mate(t, k):
        push(tile(same[k], order[t]), w_s, ymt_r.at[t], {"col": mate}).start()

    def along_y(d, k):
        push(tile(same[k], y), w_s, yin_r.at[k // 3], {"row": at(0, (yu, yd)[d])}).start()

    for k in range(3):
        along_x(0, k).start()
    to_mate(0, 0)

    rid = lax.broadcasted_iota(jnp.int32, (FW, FW), 1)
    fid = lax.broadcasted_iota(jnp.int32, (FW, FW), 0)
    inner = lax.rem(rid, 256)
    slot = (inner // 16) * 4 + lax.rem(inner, 4)
    upper = jnp.where(slot == 0, 64, GRP - slot)
    want = lax.rem(inner // 4, 4) * GRP + jnp.where(rid < 256, slot, upper)
    perm = jnp.where(fid == want, 1.0, 0.0).astype(BF)
    loads[1].wait()
    blk[...] = jnp.dot(pblk[...], perm, preferred_element_type=F32).astype(BF)

    half = pl.ds(pl.multiple_of(core * 16, 16), 16)
    quarter = pl.ds(pl.multiple_of(x * GRP, GRP), GRP)

    def mine(yy, c=None):
        c = col if c is None else c
        return pt.at[yy, :, pl.ds(pl.multiple_of(lax.rem(c, 2) * 16, 16), 16), pl.ds(pl.multiple_of((c // 2) * GRP, GRP), GRP)]

    own = pltpu.make_async_copy(blk.at[half, quarter], pt.at[y, z, half, quarter], ld.at[4])
    own.start()

    def pz_send(dz):
        pltpu.make_async_remote_copy(src_ref=blk.at[half, quarter], dst_ref=pt.at[y, z, half, quarter], send_sem=pz_s, recv_sem=pz_r, device_id={"row": at(dz, y)}, device_id_type=MESH).start()

    pl.semaphore_wait(hops.at[0], 4)
    tell(1, (at(2, y), at(NZ - 2, y)))
    for dz in (1, 15, 2, 14):
        pz_send(dz)

    arrived(928, ld.at[3])
    lane = lax.rem(lax.broadcasted_iota(jnp.int32, (2 * LOC, 4 * LOC), 1), 4)
    sub = lax.rem(lax.broadcasted_iota(jnp.int32, (256, 256), 0), 4)
    for s in range(4):
        m1[s] = first[...] * jnp.where(lane == s, 1.0, 0.0).astype(BF)
        l3[s] = last[...] * jnp.where(sub == s, 1.0, 0.0).astype(BF)

    pl.semaphore_wait(hops.at[1], 2)
    tell(2, (at(4, y), at(NZ - 4, y)))
    for dz in (3, 13, 4, 12):
        pz_send(dz)

    for k in range(3):
        arrived(64, pin_r.at[k])
        to_mate(0, k + 1)
        along_y(0, k + 1)
        along_y(1, k + 1)
        if k == 1:
            for j in range(3):
                along_x(1, j).start()
            for t in range(1, 4):
                to_mate(t, 0)

    pl.semaphore_wait(hops.at[2], 2)
    tell(3, (at(0, yu), at(0, yd), at(0, yo)))
    for dz in (8, 7, 9, 6, 10, 5, 11):
        pz_send(dz)
    own.wait()
    loads[2].wait()

    def far(i):
        step = (i + 1) // 2
        return lax.rem(8 + step * (1 - 2 * lax.rem(i, 2)) + NZ, NZ)

    def px(u, k):
        c = (col, col, col, col, xl * 2 + core, xr * 2 + core, xo * 2 + core)[k]
        peer = (right, left, xo * 2 + core, mate, mate, mate, mate)[k]
        push(mine(order[u], c), p_s, px_r.at[u if k < 3 else 4], {"col": peer}).start()

    def px_out(u):
        for k in range(4):
            px(u, k)

    for t in range(GROUPS):
        g = order[t]
        if t == 1:
            pl.semaphore_wait(hops.at[3], 3)
            arrived(192, pin_r.at[3])
            for k in (1, 2, 3):
                to_mate(1, k)
            arrived(256, yin_r.at[0])
            for k in (1, 2):
                to_mate(2, k)
                to_mate(3, k)
        if t == 2:
            arrived(128, yin_r.at[1])
            to_mate(2, 3)
            to_mate(3, 3)
            part = pt.at[y, pl.ds(0, NZ - 1), half, quarter]
            pltpu.make_async_copy(part, part, pz_r).wait()
            for o in range(3):
                push(mine(y), p_s, py_r, {"row": at(0, order[o + 1])}).start()
            px_out(0)
        arrived(256, ymt_r.at[t])
        w = wfull[:, pl.ds(pl.multiple_of(g * GRP, GRP), GRP)]
        mapped = jnp.dot(tok[...], w, preferred_element_type=F32).astype(BF)
        zero = jnp.zeros((64, GRP), BF)
        parts = []
        for m in range(3):
            piece = mapped[64 * m : 64 * m + 64]
            parts.append(jnp.concatenate([piece, zero], 1))
            parts.append(jnp.concatenate([zero, piece], 1))
        spread = bdot(chan[...], jnp.concatenate(parts, 0))
        for m in range(3):
            snd[t, :, m] = spread[:, GRP * m : GRP * m + GRP].reshape(NZ, 4, GRP).astype(BF)

        def a1_send(i, c, t=t, g=g):
            to = lax.rem(z + far(i), NZ)
            pltpu.make_async_remote_copy(src_ref=snd.at[t, to], dst_ref=dat.at[row], send_sem=a1_s, recv_sem=a1_r, device_id={"row": to * NY + g}, device_id_type=MESH).start()
            return c

        lax.fori_loop(0, NZ - 1 if t == 0 else NZ, a1_send, 0)
        if t == 0:
            pltpu.make_async_copy(snd.at[0, z], dat.at[row], a1_r).start()

    arrived(192, py_r)
    for u in (1, 2, 3):
        px_out(u)

    pltpu.make_async_copy(dat, dat, a1_r).wait()
    data = dat[...].reshape(4 * LOC, GRP)
    cc, sn = twist[0], twist[1]
    first_slot = z == 0
    lanes = lax.broadcasted_iota(jnp.int32, (1, GRP), 1) < 64
    sgn = jnp.where(lanes, 1.0, -1.0)
    zero_b = jnp.where(lanes, 1.0, 0.0)
    spec = jnp.where(first_slot, 1.0, 0.0)
    outs = [None] * 3
    for s in range(4):
        got = jnp.dot(m1[s], data, preferred_element_type=F32)
        re, im = got[:LOC], got[LOC:]
        tre = re * cc - im * sn
        tim = re * sn + im * cc
        if s == 0:
            lo_mask = zero_b * spec + sgn * (1.0 - spec)
            up_keep, up_turn = 1.0 - spec, zero_b * spec
            lo_re, lo_im = tre * lo_mask, tim * lo_mask
            up_re = tre * up_keep + pltpu.roll(tre, 64, 1) * up_turn
            up_im = tim * up_keep + pltpu.roll(tim, 64, 1) * up_turn
        else:
            lo_re, lo_im, up_re, up_im = tre * sgn, tim * sgn, tre, tim
        lo = jnp.concatenate([lo_re, lo_im], 1).astype(BF)
        up = jnp.concatenate([up_re, up_im], 1).astype(BF)
        for m in range(3):
            rhs = jnp.concatenate([lo[64 * m : 64 * m + 64], up[64 * m : 64 * m + 64]], 0)
            term = bdot(l3[s], rhs)
            outs[m] = term if outs[m] is None else outs[m] + term
    for m in range(3):
        snd2[:, m] = outs[m].reshape(ROWS, 4, GRP).astype(BF)

    pltpu.make_async_copy(snd2.at[row], dat2.at[row], a2_r).start()

    def a2_send(i, c):
        to = at(far(i // NY), lax.rem(y + lax.rem(i + 1, NY), NY))
        pltpu.make_async_remote_copy(src_ref=snd2.at[to], dst_ref=dat2.at[row], send_sem=a2_s, recv_sem=a2_r, device_id={"row": to}, device_id_type=MESH).start()
        return c

    lax.fori_loop(0, ROWS - 1, a2_send, 0)

    for u in range(4):
        arrived(192, px_r.at[u])
        for k in (4, 5, 6):
            px(u, k)

    arrived(28 * 64, w_s)
    pltpu.make_async_copy(part, part, pz_s).wait()
    arrived(31 * 64, p_s)
    for sem in (a1_s, a2_s):
        pltpu.make_async_copy(dat.at[pl.ds(0, ROWS - 1)], dat.at[pl.ds(0, ROWS - 1)], sem).wait()
    arrived(1024, px_r.at[4])

    pltpu.make_async_copy(dat2, dat2, a2_r).wait()
    sides = []
    for m in range(3):
        t = dat2[:, m].reshape(256, GRP).T
        sides.append(jnp.concatenate([t[:64], t[64:]], 1))
    lhs = jnp.concatenate(sides, 0)
    lhs_ref[...] = lhs


def product(lhs_ref, pt_ref, out_hbm, out, sem):
    wide = D // 8
    copies = []
    for n in range(8):
        cols = pl.ds(wide * n, wide)
        rhs = jnp.concatenate([pt_ref[yy, zz] for zz in (2 * n, 2 * n + 1) for yy in range(NY)], 0)
        out[:, cols] = bdot(lhs_ref[...], rhs).astype(BF)
        copies.append(pltpu.make_async_copy(out.at[:, cols], out_hbm.at[0, :, cols], sem.at[n]))
        copies[-1].start()
    for c in copies:
        c.wait()


def shards(tokens, proj_in, proj_out):
    chan, first, twist, last = tables()
    anyspec = pl.BlockSpec(memory_space=pltpu.HBM)
    dma = pltpu.SemaphoreType.DMA
    lhs, pt = pl.pallas_call(
        kernel,
        out_shape=(jax.ShapeDtypeStruct((LOC, FW), BF), jax.ShapeDtypeStruct((NY, NZ, 32, FW), BF)),
        in_specs=[anyspec] * 7,
        out_specs=(pl.BlockSpec(memory_space=pltpu.VMEM), pl.BlockSpec(memory_space=pltpu.VMEM)),
        scratch_shapes=[
            pltpu.VMEM((LOC, D), BF),
            pltpu.VMEM((D, FW), BF),
            pltpu.VMEM((32, FW), BF),
            pltpu.VMEM((64, 256), BF),
            pltpu.VMEM((2 * LOC, 4 * LOC), BF),
            pltpu.VMEM((2, LOC, GRP), F32),
            pltpu.VMEM((256, 256), BF),
            pltpu.VMEM((4, 2 * LOC, 4 * LOC), BF),
            pltpu.VMEM((4, 256, 256), BF),
            pltpu.VMEM((32, FW), BF),
            pltpu.VMEM((GROUPS, NZ, 3, 4, GRP), BF),
            pltpu.VMEM((ROWS, 3, 4, GRP), BF),
            pltpu.VMEM((ROWS, 3, 4, GRP), BF),
            pltpu.VMEM((ROWS, 3, 4, GRP), BF),
            dma((5,)),
            pltpu.SemaphoreType.REGULAR((4,)),
            dma,
            dma((4,)),
            dma((2,)),
            dma((4,)),
            dma,
            dma,
            dma,
            dma,
            dma,
            dma,
            dma,
            dma,
            dma((5,)),
        ],
        compiler_params=pltpu.CompilerParams(collective_id=0, has_side_effects=True, vmem_limit_bytes=24 << 20),
    )(
        *(
            pltpu.with_memory_space_constraint(a, pltpu.HBM)
            for a in (tokens, proj_in, proj_out.T, jnp.asarray(chan, BF), jnp.asarray(first, BF), jnp.asarray(twist, F32), jnp.asarray(last, BF))
        )
    )
    return pl.pallas_call(
        product,
        out_shape=jax.ShapeDtypeStruct((1, LOC, D), BF),
        in_specs=[pl.BlockSpec(memory_space=pltpu.VMEM)] * 2,
        out_specs=pl.BlockSpec(memory_space=pl.ANY),
        scratch_shapes=[pltpu.VMEM((LOC, D), BF), dma((8,))],
        compiler_params=pltpu.CompilerParams(vmem_limit_bytes=24 << 20),
    )(lhs, pt)


def solution(mesh):
    return jax.shard_map(
        shards,
        mesh=mesh,
        in_specs=(P("col", "row", None), P("col", None), P(None, "row")),
        out_specs=P("col", "row", None),
        check_vma=False,
    )
```

```python
import math

import jax
import jax.numpy as jnp
import numpy as np
from jax import lax
from jax.experimental import pallas as pl
from jax.experimental.pallas import tpu as pltpu
from jax.sharding import PartitionSpec as P

MESH = pl.DeviceIdType.MESH
GRP = 128
GROUPS = 4
NZ, NY, NX = 16, 4, 4
ROWS = NZ * NY
LOC = 192
LEN = ROWS * LOC
D = 2048
KS = 256
FW = GROUPS * GRP
F32 = jnp.float32
BF = jnp.bfloat16


def tables():
    s = np.arange(64)[:, None]
    f = np.arange(GRP)[None, :]
    ang = 2 * np.pi * ((s * f) % GRP) / GRP
    part_a = np.cos(ang)
    part_b = np.sin(ang)
    part_b[0] = np.cos(np.pi * np.arange(GRP))
    chan = np.concatenate([part_a, part_b], 1)
    q = np.arange(LOC)[:, None]
    halves = []
    for e in range(2):
        p1 = np.array([3 * (NY * zz + e + 2 * h) + m for h in range(2) for zz in range(NZ) for m in range(3)])[None, :]
        ang = 2 * np.pi * ((q * p1) % LOC) / LOC
        halves.append(np.repeat(np.concatenate([np.cos(ang), np.sin(ang)], 0), 4, axis=1))
    first = np.stack(halves)
    q2 = np.arange(64)[None, :]
    ang = 2 * np.pi * ((q * q2) % LEN) / LEN
    scale = 1.0 / math.sqrt(GRP * LEN)
    twist = np.stack([np.tile(np.cos(ang), (1, 2)), np.tile(np.sin(ang), (1, 2))]) * scale
    r = np.arange(64)[:, None]
    ang = 2 * np.pi * ((r * q2) % 64) / 64
    c, n = np.cos(ang), np.sin(ang)
    last = np.repeat(np.concatenate([c, n, -n, c], 1), 4, axis=0)
    return chan, first, twist, last


def bdot(a, b):
    return lax.dot_general(a, b, (((1,), (1,)), ((), ())), preferred_element_type=F32)


def kernel(tok_hbm, win_hbm, pout_hbm, chan_hbm, first_hbm, twist_hbm, last_hbm, lhs_ref, pt, tok, wfull, pblk, chan, first, twist, last, m1, l3, blk, snd, acc, dat, snd2, dat2, ld, hops, w_s, pin_r, yin_r, ymt_r, a1_s, a1_r, a2_s, a2_r, pz_s, pz_r, p_s, py_r, px_r):
    row = lax.axis_index("row")
    col = lax.axis_index("col")
    z, y = row // NY, lax.rem(row, NY)
    x, core = col // 2, lax.rem(col, 2)
    xr = lax.rem(x + 1, NX)
    xl = lax.rem(x + NX - 1, NX)
    xo = lax.rem(x + 2, NX)
    right, left, mate = xr * 2 + core, xl * 2 + core, x * 2 + (1 - core)
    yu, yd, yo = lax.rem(y + 1, NY), lax.rem(y + NY - 1, NY), lax.rem(y + 2, NY)

    def at(dz, yy):
        return lax.rem(z + dz, NZ) * NY + yy

    bar = pltpu.get_barrier_semaphore()
    for peer in (right, left, xo * 2 + core, mate):
        pl.semaphore_signal(bar, inc=1, device_id={"col": peer}, device_id_type=MESH)
    for peer in (at(0, yu), at(0, yd), at(1, y), at(NZ - 1, y)):
        pl.semaphore_signal(bar, inc=1, device_id={"row": peer}, device_id_type=MESH)

    loads = [
        pltpu.make_async_copy(win_hbm, wfull.at[pl.ds(pl.multiple_of(col * KS, KS), KS), :], ld.at[0]),
        pltpu.make_async_copy(pout_hbm, pblk, ld.at[1]),
        pltpu.make_async_copy(tok_hbm.at[0], tok, ld.at[2]),
        pltpu.make_async_copy(chan_hbm, chan, ld.at[3]),
        pltpu.make_async_copy(first_hbm, first, ld.at[3]),
        pltpu.make_async_copy(last_hbm, last, ld.at[3]),
        pltpu.make_async_copy(twist_hbm, twist, ld.at[3]),
    ]
    for c in loads:
        c.start()
    pl.semaphore_wait(bar, 8)

    def tell(i, peers):
        for peer in peers:
            pl.semaphore_signal(hops.at[i], inc=1, device_id={"row": peer}, device_id_type=MESH)

    tell(0, (at(1, y), at(NZ - 1, y), at(0, yu), at(0, yd)))
    loads[0].wait()

    same = [col, xl * 2 + core, xr * 2 + core, xo * 2 + core]

    def tile(c, g):
        return wfull.at[pl.ds(pl.multiple_of(c * KS, KS), KS), pl.ds(pl.multiple_of(g * GRP, GRP), GRP)]

    def arrived(rows, sem):
        pltpu.make_async_copy(wfull.at[pl.ds(0, rows)], wfull.at[pl.ds(0, rows)], sem).wait()

    def push(ref, ss, rs, peer):
        return pltpu.make_async_remote_copy(src_ref=ref, dst_ref=ref, send_sem=ss, recv_sem=rs, device_id=peer, device_id_type=MESH)

    order = (y, yo, yu, yd)

    def along_x(t, k):
        return push(tile(col, order[t]), w_s, pin_r.at[k if t == 0 else 3], {"col": (right, left, xo * 2 + core)[k]})

    def to_mate(t, k):
        push(tile(same[k], order[t]), w_s, ymt_r.at[t], {"col": mate}).start()

    def along_y(d, k):
        push(tile(same[k], y), w_s, yin_r.at[k // 3], {"row": at(0, (yu, yd)[d])}).start()

    for k in range(3):
        along_x(0, k).start()
    to_mate(0, 0)

    rid = lax.broadcasted_iota(jnp.int32, (FW, FW), 1)
    fid = lax.broadcasted_iota(jnp.int32, (FW, FW), 0)
    inner = lax.rem(rid, 256)
    slot = (inner // 16) * 4 + lax.rem(inner, 4)
    upper = jnp.where(slot == 0, 64, GRP - slot)
    want = lax.rem(inner // 4, 4) * GRP + jnp.where(rid < 256, slot, upper)
    perm = jnp.where(fid == want, 1.0, 0.0).astype(BF)
    loads[1].wait()
    blk[...] = jnp.dot(pblk[...], perm, preferred_element_type=F32).astype(BF)

    half = pl.ds(pl.multiple_of(core * 16, 16), 16)
    quarter = pl.ds(pl.multiple_of(x * GRP, GRP), GRP)

    def mine(yy, c=None):
        c = col if c is None else c
        return pt.at[yy, :, pl.ds(pl.multiple_of(lax.rem(c, 2) * 16, 16), 16), pl.ds(pl.multiple_of((c // 2) * GRP, GRP), GRP)]

    own = pltpu.make_async_copy(blk.at[half, quarter], pt.at[y, z, half, quarter], ld.at[4])
    own.start()

    def pz_send(dz):
        pltpu.make_async_remote_copy(src_ref=blk.at[half, quarter], dst_ref=pt.at[y, z, half, quarter], send_sem=pz_s, recv_sem=pz_r, device_id={"row": at(dz, y)}, device_id_type=MESH).start()

    pl.semaphore_wait(hops.at[0], 4)
    tell(1, (at(2, y), at(NZ - 2, y)))
    for dz in (1, 15, 2, 14):
        pz_send(dz)

    arrived(928, ld.at[3])
    lane = lax.rem(lax.broadcasted_iota(jnp.int32, (2 * LOC, 2 * LOC), 1), 4)
    sub = lax.rem(lax.broadcasted_iota(jnp.int32, (256, 256), 0), 4)
    for s in range(4):
        for e in range(2):
            m1[e, s] = first[e] * jnp.where(lane == s, 1.0, 0.0).astype(BF)
        l3[s] = last[...] * jnp.where(sub == s, 1.0, 0.0).astype(BF)

    pl.semaphore_wait(hops.at[1], 2)
    tell(2, (at(4, y), at(NZ - 4, y)))
    for dz in (3, 13, 4, 12):
        pz_send(dz)

    for k in range(3):
        arrived(64, pin_r.at[k])
        to_mate(0, k + 1)
        along_y(0, k + 1)
        along_y(1, k + 1)
        if k == 1:
            for j in range(3):
                along_x(1, j).start()
            for t in range(1, 4):
                to_mate(t, 0)

    pl.semaphore_wait(hops.at[2], 2)
    tell(3, (at(0, yu), at(0, yd), at(0, yo)))
    for dz in (8, 7, 9, 6, 10, 5, 11):
        pz_send(dz)
    own.wait()
    loads[2].wait()

    def far(i):
        step = (i + 1) // 2
        return lax.rem(8 + step * (1 - 2 * lax.rem(i, 2)) + NZ, NZ)

    def px(u, k):
        c = (col, col, col, col, xl * 2 + core, xr * 2 + core, xo * 2 + core)[k]
        peer = (right, left, xo * 2 + core, mate, mate, mate, mate)[k]
        push(mine(order[u], c), p_s, px_r.at[u if k < 3 else 4], {"col": peer}).start()

    def px_out(u):
        for k in range(4):
            px(u, k)

    side = lax.rem(y, 2)

    def groups_out(t, which):
        def send():
            def a1_send(i, c):
                to = lax.rem(z + far(i), NZ)
                pltpu.make_async_remote_copy(src_ref=snd.at[t, to], dst_ref=dat.at[side, y // 2, z], send_sem=a1_s, recv_sem=a1_r.at[t // 2], device_id={"row": to * NY + order[t]}, device_id_type=MESH).start()
                return c

            lax.fori_loop(0, NZ - 1 if t == 0 else NZ, a1_send, 0)
            if t == 0:
                pltpu.make_async_copy(snd.at[0, z], dat.at[side, y // 2, z], a1_r.at[0]).start()

        if which is None:
            send()
        else:
            pl.when(core == which)(send)

    for t in range(GROUPS):
        g = order[t]
        if t == 1:
            pl.semaphore_wait(hops.at[3], 3)
            arrived(192, pin_r.at[3])
            for k in (1, 2, 3):
                to_mate(1, k)
            arrived(256, yin_r.at[0])
            for k in (1, 2):
                to_mate(2, k)
                to_mate(3, k)
        if t == 2:
            arrived(128, yin_r.at[1])
            to_mate(2, 3)
            to_mate(3, 3)
            part = pt.at[y, pl.ds(0, NZ - 1), half, quarter]
            pltpu.make_async_copy(part, part, pz_r).wait()
            for o in range(3):
                push(mine(y), p_s, py_r, {"row": at(0, order[o + 1])}).start()
            px_out(0)
        arrived(256, ymt_r.at[t])
        w = wfull[:, pl.ds(pl.multiple_of(g * GRP, GRP), GRP)]
        mapped = jnp.dot(tok[...], w, preferred_element_type=F32).astype(BF)
        zero = jnp.zeros((64, GRP), BF)
        parts = []
        for m in range(3):
            piece = mapped[64 * m : 64 * m + 64]
            parts.append(jnp.concatenate([piece, zero], 1))
            parts.append(jnp.concatenate([zero, piece], 1))
        spread = bdot(chan[...], jnp.concatenate(parts, 0))
        for m in range(3):
            snd[t, :, m] = spread[:, GRP * m : GRP * m + GRP].reshape(NZ, 4, GRP).astype(BF)

        for u in range(GROUPS):
            early, late = u == t, t == min(u + 1, GROUPS - 1)
            if early or late:
                which = None if early and late else 1 if early else 0
                groups_out(u, which)

    arrived(192, py_r)
    for u in (1, 2, 3):
        px_out(u)

    early = dat.at[side]
    pltpu.make_async_copy(early, early, a1_r.at[0]).wait()
    data = early[...].reshape(2 * LOC, GRP)
    for s in range(4):
        acc[s] = jnp.dot(m1[side, s], data, preferred_element_type=F32)
    late = dat.at[1 - side]
    pltpu.make_async_copy(late, late, a1_r.at[1]).wait()
    data = late[...].reshape(2 * LOC, GRP)
    cc, sn = twist[0], twist[1]
    first_slot = z == 0
    lanes = lax.broadcasted_iota(jnp.int32, (1, GRP), 1) < 64
    sgn = jnp.where(lanes, 1.0, -1.0)
    zero_b = jnp.where(lanes, 1.0, 0.0)
    spec = jnp.where(first_slot, 1.0, 0.0)
    outs = [None] * 3
    for s in range(4):
        got = acc[s] + jnp.dot(m1[1 - side, s], data, preferred_element_type=F32)
        re, im = got[:LOC], got[LOC:]
        tre = re * cc - im * sn
        tim = re * sn + im * cc
        if s == 0:
            lo_mask = zero_b * spec + sgn * (1.0 - spec)
            up_keep, up_turn = 1.0 - spec, zero_b * spec
            lo_re, lo_im = tre * lo_mask, tim * lo_mask
            up_re = tre * up_keep + pltpu.roll(tre, 64, 1) * up_turn
            up_im = tim * up_keep + pltpu.roll(tim, 64, 1) * up_turn
        else:
            lo_re, lo_im, up_re, up_im = tre * sgn, tim * sgn, tre, tim
        lo = jnp.concatenate([lo_re, lo_im], 1).astype(BF)
        up = jnp.concatenate([up_re, up_im], 1).astype(BF)
        for m in range(3):
            rhs = jnp.concatenate([lo[64 * m : 64 * m + 64], up[64 * m : 64 * m + 64]], 0)
            term = bdot(l3[s], rhs)
            outs[m] = term if outs[m] is None else outs[m] + term
    for m in range(3):
        snd2[:, m] = outs[m].reshape(ROWS, 4, GRP).astype(BF)

    pltpu.make_async_copy(snd2.at[row], dat2.at[row], a2_r).start()

    def a2_send(i, c):
        to = at(far(i // NY), lax.rem(y + lax.rem(i + 1, NY), NY))
        pltpu.make_async_remote_copy(src_ref=snd2.at[to], dst_ref=dat2.at[row], send_sem=a2_s, recv_sem=a2_r, device_id={"row": to}, device_id_type=MESH).start()
        return c

    lax.fori_loop(0, ROWS - 1, a2_send, 0)

    for u in range(4):
        arrived(192, px_r.at[u])
        for k in (4, 5, 6):
            px(u, k)

    arrived(28 * 64, w_s)
    pltpu.make_async_copy(part, part, pz_s).wait()
    arrived(31 * 64, p_s)
    for sem in (a1_s, a2_s):
        pltpu.make_async_copy(dat2.at[pl.ds(0, ROWS - 1)], dat2.at[pl.ds(0, ROWS - 1)], sem).wait()
    arrived(1024, px_r.at[4])

    pltpu.make_async_copy(dat2, dat2, a2_r).wait()
    sides = []
    for m in range(3):
        t = dat2[:, m].reshape(256, GRP).T
        sides.append(jnp.concatenate([t[:64], t[64:]], 1))
    lhs = jnp.concatenate(sides, 0)
    lhs_ref[...] = lhs


def product(lhs_ref, pt_ref, out_hbm, out, sem):
    wide = D // 8
    copies = []
    for n in range(8):
        cols = pl.ds(wide * n, wide)
        rhs = jnp.concatenate([pt_ref[yy, zz] for zz in (2 * n, 2 * n + 1) for yy in range(NY)], 0)
        out[:, cols] = bdot(lhs_ref[...], rhs).astype(BF)
        copies.append(pltpu.make_async_copy(out.at[:, cols], out_hbm.at[0, :, cols], sem.at[n]))
        copies[-1].start()
    for c in copies:
        c.wait()


def shards(tokens, proj_in, proj_out):
    chan, first, twist, last = tables()
    anyspec = pl.BlockSpec(memory_space=pltpu.HBM)
    dma = pltpu.SemaphoreType.DMA
    lhs, pt = pl.pallas_call(
        kernel,
        out_shape=(jax.ShapeDtypeStruct((LOC, FW), BF), jax.ShapeDtypeStruct((NY, NZ, 32, FW), BF)),
        in_specs=[anyspec] * 7,
        out_specs=(pl.BlockSpec(memory_space=pltpu.VMEM), pl.BlockSpec(memory_space=pltpu.VMEM)),
        scratch_shapes=[
            pltpu.VMEM((LOC, D), BF),
            pltpu.VMEM((D, FW), BF),
            pltpu.VMEM((32, FW), BF),
            pltpu.VMEM((64, 256), BF),
            pltpu.VMEM((2, 2 * LOC, 2 * LOC), BF),
            pltpu.VMEM((2, LOC, GRP), F32),
            pltpu.VMEM((256, 256), BF),
            pltpu.VMEM((2, 4, 2 * LOC, 2 * LOC), BF),
            pltpu.VMEM((4, 256, 256), BF),
            pltpu.VMEM((32, FW), BF),
            pltpu.VMEM((GROUPS, NZ, 3, 4, GRP), BF),
            pltpu.VMEM((4, 2 * LOC, GRP), F32),
            pltpu.VMEM((2, 2, NZ, 3, 4, GRP), BF),
            pltpu.VMEM((ROWS, 3, 4, GRP), BF),
            pltpu.VMEM((ROWS, 3, 4, GRP), BF),
            dma((5,)),
            pltpu.SemaphoreType.REGULAR((4,)),
            dma,
            dma((4,)),
            dma((2,)),
            dma((4,)),
            dma,
            dma((2,)),
            dma,
            dma,
            dma,
            dma,
            dma,
            dma,
            dma((5,)),
        ],
        compiler_params=pltpu.CompilerParams(collective_id=0, has_side_effects=True, vmem_limit_bytes=24 << 20),
    )(
        *(
            pltpu.with_memory_space_constraint(a, pltpu.HBM)
            for a in (tokens, proj_in, proj_out.T, jnp.asarray(chan, BF), jnp.asarray(first, BF), jnp.asarray(twist, F32), jnp.asarray(last, BF))
        )
    )
    return pl.pallas_call(
        product,
        out_shape=jax.ShapeDtypeStruct((1, LOC, D), BF),
        in_specs=[pl.BlockSpec(memory_space=pltpu.VMEM)] * 2,
        out_specs=pl.BlockSpec(memory_space=pl.ANY),
        scratch_shapes=[pltpu.VMEM((LOC, D), BF), dma((8,))],
        compiler_params=pltpu.CompilerParams(vmem_limit_bytes=24 << 20),
    )(lhs, pt)


def solution(mesh):
    return jax.shard_map(
        shards,
        mesh=mesh,
        in_specs=(P("col", "row", None), P("col", None), P(None, "row")),
        out_specs=P("col", "row", None),
        check_vma=False,
    )
```

```python
import math

import jax
import jax.numpy as jnp
import numpy as np
from jax import lax
from jax.experimental import pallas as pl
from jax.experimental.pallas import tpu as pltpu
from jax.sharding import PartitionSpec as P

MESH = pl.DeviceIdType.MESH
GRP = 128
GROUPS = 4
NZ, NY, NX = 16, 4, 4
ROWS = NZ * NY
LOC = 192
LEN = ROWS * LOC
D = 2048
KS = 256
FW = GROUPS * GRP
F32 = jnp.float32
BF = jnp.bfloat16


def tables():
    s = np.arange(64)[:, None]
    f = np.arange(GRP)[None, :]
    ang = 2 * np.pi * ((s * f) % GRP) / GRP
    part_a = np.cos(ang)
    part_b = np.sin(ang)
    part_b[0] = np.cos(np.pi * np.arange(GRP))
    chan = np.concatenate([part_a, part_b], 1)
    q = np.arange(LOC)[:, None]
    halves = []
    for e in range(2):
        p1 = np.array([3 * (NY * zz + e + 2 * h) + m for h in range(2) for zz in range(NZ) for m in range(3)])[None, :]
        ang = 2 * np.pi * ((q * p1) % LOC) / LOC
        halves.append(np.repeat(np.concatenate([np.cos(ang), np.sin(ang)], 0), 4, axis=1))
    first = np.stack(halves)
    q2 = np.arange(64)[None, :]
    ang = 2 * np.pi * ((q * q2) % LEN) / LEN
    scale = 1.0 / math.sqrt(GRP * LEN)
    twist = np.stack([np.tile(np.cos(ang), (1, 2)), np.tile(np.sin(ang), (1, 2))]) * scale
    r = np.arange(64)[:, None]
    ang = 2 * np.pi * ((r * q2) % 64) / 64
    c, n = np.cos(ang), np.sin(ang)
    last = np.repeat(np.concatenate([c, n, -n, c], 1), 4, axis=0)
    return chan, first, twist, last


def bdot(a, b):
    return lax.dot_general(a, b, (((1,), (1,)), ((), ())), preferred_element_type=F32)


def kernel(tok_hbm, win_hbm, pout_hbm, chan_hbm, first_hbm, twist_hbm, last_hbm, lhs_ref, pt, tok, wfull, pblk, chan, first, twist, last, m1, l3, blk, snd, acc, dat, snd2, dat2, ld, hops, w_s, pin_r, yin_r, ymt_r, a1_s, a1_r, a2_s, a2_r, pz_s, pz_r, p_s, py_r, px_r):
    row = lax.axis_index("row")
    col = lax.axis_index("col")
    z, y = row // NY, lax.rem(row, NY)
    x, core = col // 2, lax.rem(col, 2)
    xr = lax.rem(x + 1, NX)
    xl = lax.rem(x + NX - 1, NX)
    xo = lax.rem(x + 2, NX)
    right, left, mate = xr * 2 + core, xl * 2 + core, x * 2 + (1 - core)
    yu, yd, yo = lax.rem(y + 1, NY), lax.rem(y + NY - 1, NY), lax.rem(y + 2, NY)

    def at(dz, yy):
        return lax.rem(z + dz, NZ) * NY + yy

    bar = pltpu.get_barrier_semaphore()
    for peer in (right, left, xo * 2 + core, mate):
        pl.semaphore_signal(bar, inc=1, device_id={"col": peer}, device_id_type=MESH)
    for peer in (at(0, yu), at(0, yd), at(1, y), at(NZ - 1, y)):
        pl.semaphore_signal(bar, inc=1, device_id={"row": peer}, device_id_type=MESH)

    loads = [
        pltpu.make_async_copy(win_hbm, wfull.at[pl.ds(pl.multiple_of(col * KS, KS), KS), :], ld.at[0]),
        pltpu.make_async_copy(pout_hbm, pblk, ld.at[1]),
        pltpu.make_async_copy(tok_hbm.at[0], tok, ld.at[2]),
        pltpu.make_async_copy(chan_hbm, chan, ld.at[3]),
        pltpu.make_async_copy(first_hbm, first, ld.at[3]),
        pltpu.make_async_copy(last_hbm, last, ld.at[3]),
        pltpu.make_async_copy(twist_hbm, twist, ld.at[3]),
    ]
    for c in loads:
        c.start()
    pl.semaphore_wait(bar, 8)

    def tell(i, peers):
        for peer in peers:
            pl.semaphore_signal(hops.at[i], inc=1, device_id={"row": peer}, device_id_type=MESH)

    tell(0, (at(1, y), at(NZ - 1, y), at(0, yu), at(0, yd)))
    loads[0].wait()

    same = [col, xl * 2 + core, xr * 2 + core, xo * 2 + core]

    def tile(c, g):
        return wfull.at[pl.ds(pl.multiple_of(c * KS, KS), KS), pl.ds(pl.multiple_of(g * GRP, GRP), GRP)]

    def arrived(rows, sem):
        pltpu.make_async_copy(wfull.at[pl.ds(0, rows)], wfull.at[pl.ds(0, rows)], sem).wait()

    def push(ref, ss, rs, peer):
        return pltpu.make_async_remote_copy(src_ref=ref, dst_ref=ref, send_sem=ss, recv_sem=rs, device_id=peer, device_id_type=MESH)

    order = (y, yo, yu, yd)

    def along_x(t, k):
        return push(tile(col, order[t]), w_s, pin_r.at[k if t == 0 else 3], {"col": (right, left, xo * 2 + core)[k]})

    def to_mate(t, k):
        push(tile(same[k], order[t]), w_s, ymt_r.at[t], {"col": mate}).start()

    def along_y(d, k):
        push(tile(same[k], y), w_s, yin_r.at[k // 3], {"row": at(0, (yu, yd)[d])}).start()

    for k in range(3):
        along_x(0, k).start()
    to_mate(0, 0)

    rid = lax.broadcasted_iota(jnp.int32, (FW, FW), 1)
    fid = lax.broadcasted_iota(jnp.int32, (FW, FW), 0)
    inner = lax.rem(rid, 256)
    slot = (inner // 16) * 4 + lax.rem(inner, 4)
    upper = jnp.where(slot == 0, 64, GRP - slot)
    want = lax.rem(inner // 4, 4) * GRP + jnp.where(rid < 256, slot, upper)
    perm = jnp.where(fid == want, 1.0, 0.0).astype(BF)
    loads[1].wait()
    blk[...] = jnp.dot(pblk[...], perm, preferred_element_type=F32).astype(BF)

    half = pl.ds(pl.multiple_of(core * 16, 16), 16)
    quarter = pl.ds(pl.multiple_of(x * GRP, GRP), GRP)

    def mine(yy, c=None):
        c = col if c is None else c
        return pt.at[yy, :, pl.ds(pl.multiple_of(lax.rem(c, 2) * 16, 16), 16), pl.ds(pl.multiple_of((c // 2) * GRP, GRP), GRP)]

    own = pltpu.make_async_copy(blk.at[half, quarter], pt.at[y, z, half, quarter], ld.at[4])
    own.start()

    def pz_send(dz):
        rs = pz_r.at[{4: 1, 12: 2}.get(dz, 0)]
        pltpu.make_async_remote_copy(src_ref=blk.at[half, quarter], dst_ref=pt.at[y, z, half, quarter], send_sem=pz_s, recv_sem=rs, device_id={"row": at(dz, y)}, device_id_type=MESH).start()

    def pz_relay(i):
        ref = pt.at[y, lax.rem(z + (12, 4)[i], NZ), half, quarter]
        pltpu.make_async_copy(ref, ref, pz_r.at[i + 1]).wait()
        for dz in ((3, 2, 1), (12, 13, 14, 15))[i]:
            push(ref, pz_s, pz_r.at[0], {"row": at(dz, y)}).start()

    pl.semaphore_wait(hops.at[0], 4)
    tell(1, (at(2, y), at(NZ - 2, y)))
    for dz in (1, 15, 2, 14):
        pz_send(dz)

    arrived(928, ld.at[3])
    lane = lax.rem(lax.broadcasted_iota(jnp.int32, (2 * LOC, 2 * LOC), 1), 4)
    sub = lax.rem(lax.broadcasted_iota(jnp.int32, (256, 256), 0), 4)
    for s in range(4):
        for e in range(2):
            m1[e, s] = first[e] * jnp.where(lane == s, 1.0, 0.0).astype(BF)
        l3[s] = last[...] * jnp.where(sub == s, 1.0, 0.0).astype(BF)

    pl.semaphore_wait(hops.at[1], 2)
    tell(2, (at(4, y), at(NZ - 4, y)))
    for dz in (3, 13, 4, 12):
        pz_send(dz)

    for k in range(3):
        arrived(64, pin_r.at[k])
        to_mate(0, k + 1)
        along_y(0, k + 1)
        along_y(1, k + 1)
        if k == 1:
            for j in range(3):
                along_x(1, j).start()
            for t in range(1, 4):
                to_mate(t, 0)

    pl.semaphore_wait(hops.at[2], 2)
    tell(3, (at(0, yu), at(0, yd), at(0, yo)))
    own.wait()
    loads[2].wait()
    for i in range(2):
        pz_relay(i)

    def far(i):
        step = (i + 1) // 2
        return lax.rem(8 + step * (1 - 2 * lax.rem(i, 2)) + NZ, NZ)

    def px(u, k):
        c = (col, col, col, col, xl * 2 + core, xr * 2 + core, xo * 2 + core)[k]
        peer = (right, left, xo * 2 + core, mate, mate, mate, mate)[k]
        push(mine(order[u], c), p_s, px_r.at[u if k < 3 else 4], {"col": peer}).start()

    def px_out(u):
        for k in range(4):
            px(u, k)

    side = lax.rem(y, 2)

    def groups_out(t, which):
        def send():
            def a1_send(i, c):
                to = lax.rem(z + far(i), NZ)
                pltpu.make_async_remote_copy(src_ref=snd.at[t, to], dst_ref=dat.at[side, y // 2, z], send_sem=a1_s, recv_sem=a1_r.at[t // 2], device_id={"row": to * NY + order[t]}, device_id_type=MESH).start()
                return c

            lax.fori_loop(0, NZ - 1 if t == 0 else NZ, a1_send, 0)
            if t == 0:
                pltpu.make_async_copy(snd.at[0, z], dat.at[side, y // 2, z], a1_r.at[0]).start()

        if which is None:
            send()
        else:
            pl.when(core == which)(send)

    for t in range(GROUPS):
        g = order[t]
        if t == 1:
            pl.semaphore_wait(hops.at[3], 3)
            arrived(192, pin_r.at[3])
            for k in (1, 2, 3):
                to_mate(1, k)
            arrived(256, yin_r.at[0])
            for k in (1, 2):
                to_mate(2, k)
                to_mate(3, k)
        if t == 2:
            arrived(128, yin_r.at[1])
            to_mate(2, 3)
            to_mate(3, 3)
            part = pt.at[y, pl.ds(0, NZ - 3), half, quarter]
            pltpu.make_async_copy(part, part, pz_r.at[0]).wait()
            for o in range(3):
                push(mine(y), p_s, py_r, {"row": at(0, order[o + 1])}).start()
            px_out(0)
        arrived(256, ymt_r.at[t])
        w = wfull[:, pl.ds(pl.multiple_of(g * GRP, GRP), GRP)]
        mapped = jnp.dot(tok[...], w, preferred_element_type=F32).astype(BF)
        zero = jnp.zeros((64, GRP), BF)
        parts = []
        for m in range(3):
            piece = mapped[64 * m : 64 * m + 64]
            parts.append(jnp.concatenate([piece, zero], 1))
            parts.append(jnp.concatenate([zero, piece], 1))
        spread = bdot(chan[...], jnp.concatenate(parts, 0))
        for m in range(3):
            snd[t, :, m] = spread[:, GRP * m : GRP * m + GRP].reshape(NZ, 4, GRP).astype(BF)

        for u in range(GROUPS):
            early, late = u == t, t == min(u + 1, GROUPS - 1)
            if early or late:
                which = None if early and late else 1 if early else 0
                groups_out(u, which)

    arrived(192, py_r)
    for u in (1, 2, 3):
        px_out(u)

    early = dat.at[side]
    pltpu.make_async_copy(early, early, a1_r.at[0]).wait()
    data = early[...].reshape(2 * LOC, GRP)
    for s in range(4):
        acc[s] = jnp.dot(m1[side, s], data, preferred_element_type=F32)
    late = dat.at[1 - side]
    pltpu.make_async_copy(late, late, a1_r.at[1]).wait()
    data = late[...].reshape(2 * LOC, GRP)
    cc, sn = twist[0], twist[1]
    first_slot = z == 0
    lanes = lax.broadcasted_iota(jnp.int32, (1, GRP), 1) < 64
    sgn = jnp.where(lanes, 1.0, -1.0)
    zero_b = jnp.where(lanes, 1.0, 0.0)
    spec = jnp.where(first_slot, 1.0, 0.0)
    outs = [None] * 3
    for s in range(4):
        got = acc[s] + jnp.dot(m1[1 - side, s], data, preferred_element_type=F32)
        re, im = got[:LOC], got[LOC:]
        tre = re * cc - im * sn
        tim = re * sn + im * cc
        if s == 0:
            lo_mask = zero_b * spec + sgn * (1.0 - spec)
            up_keep, up_turn = 1.0 - spec, zero_b * spec
            lo_re, lo_im = tre * lo_mask, tim * lo_mask
            up_re = tre * up_keep + pltpu.roll(tre, 64, 1) * up_turn
            up_im = tim * up_keep + pltpu.roll(tim, 64, 1) * up_turn
        else:
            lo_re, lo_im, up_re, up_im = tre * sgn, tim * sgn, tre, tim
        lo = jnp.concatenate([lo_re, lo_im], 1).astype(BF)
        up = jnp.concatenate([up_re, up_im], 1).astype(BF)
        for m in range(3):
            rhs = jnp.concatenate([lo[64 * m : 64 * m + 64], up[64 * m : 64 * m + 64]], 0)
            term = bdot(l3[s], rhs)
            outs[m] = term if outs[m] is None else outs[m] + term
    for m in range(3):
        snd2[:, m] = outs[m].reshape(ROWS, 4, GRP).astype(BF)

    pltpu.make_async_copy(snd2.at[row], dat2.at[row], a2_r).start()

    def a2_send(i, c):
        to = at(far(i // NY), lax.rem(y + lax.rem(i + 1, NY), NY))
        pltpu.make_async_remote_copy(src_ref=snd2.at[to], dst_ref=dat2.at[row], send_sem=a2_s, recv_sem=a2_r, device_id={"row": to}, device_id_type=MESH).start()
        return c

    lax.fori_loop(0, ROWS - 1, a2_send, 0)

    for u in range(4):
        arrived(192, px_r.at[u])
        for k in (4, 5, 6):
            px(u, k)

    arrived(28 * 64, w_s)
    part = pt.at[y, pl.ds(0, NZ - 1), half, quarter]
    pltpu.make_async_copy(part, part, pz_s).wait()
    arrived(31 * 64, p_s)
    for sem in (a1_s, a2_s):
        pltpu.make_async_copy(dat2.at[pl.ds(0, ROWS - 1)], dat2.at[pl.ds(0, ROWS - 1)], sem).wait()
    arrived(1024, px_r.at[4])

    pltpu.make_async_copy(dat2, dat2, a2_r).wait()
    sides = []
    for m in range(3):
        t = dat2[:, m].reshape(256, GRP).T
        sides.append(jnp.concatenate([t[:64], t[64:]], 1))
    lhs = jnp.concatenate(sides, 0)
    lhs_ref[...] = lhs


def product(lhs_ref, pt_ref, out_hbm, out, sem):
    wide = D // 8
    copies = []
    for n in range(8):
        cols = pl.ds(wide * n, wide)
        rhs = jnp.concatenate([pt_ref[yy, zz] for zz in (2 * n, 2 * n + 1) for yy in range(NY)], 0)
        out[:, cols] = bdot(lhs_ref[...], rhs).astype(BF)
        copies.append(pltpu.make_async_copy(out.at[:, cols], out_hbm.at[0, :, cols], sem.at[n]))
        copies[-1].start()
    for c in copies:
        c.wait()


def shards(tokens, proj_in, proj_out):
    chan, first, twist, last = tables()
    anyspec = pl.BlockSpec(memory_space=pltpu.HBM)
    dma = pltpu.SemaphoreType.DMA
    lhs, pt = pl.pallas_call(
        kernel,
        out_shape=(jax.ShapeDtypeStruct((LOC, FW), BF), jax.ShapeDtypeStruct((NY, NZ, 32, FW), BF)),
        in_specs=[anyspec] * 7,
        out_specs=(pl.BlockSpec(memory_space=pltpu.VMEM), pl.BlockSpec(memory_space=pltpu.VMEM)),
        scratch_shapes=[
            pltpu.VMEM((LOC, D), BF),
            pltpu.VMEM((D, FW), BF),
            pltpu.VMEM((32, FW), BF),
            pltpu.VMEM((64, 256), BF),
            pltpu.VMEM((2, 2 * LOC, 2 * LOC), BF),
            pltpu.VMEM((2, LOC, GRP), F32),
            pltpu.VMEM((256, 256), BF),
            pltpu.VMEM((2, 4, 2 * LOC, 2 * LOC), BF),
            pltpu.VMEM((4, 256, 256), BF),
            pltpu.VMEM((32, FW), BF),
            pltpu.VMEM((GROUPS, NZ, 3, 4, GRP), BF),
            pltpu.VMEM((4, 2 * LOC, GRP), F32),
            pltpu.VMEM((2, 2, NZ, 3, 4, GRP), BF),
            pltpu.VMEM((ROWS, 3, 4, GRP), BF),
            pltpu.VMEM((ROWS, 3, 4, GRP), BF),
            dma((5,)),
            pltpu.SemaphoreType.REGULAR((4,)),
            dma,
            dma((4,)),
            dma((2,)),
            dma((4,)),
            dma,
            dma((2,)),
            dma,
            dma,
            dma,
            dma((3,)),
            dma,
            dma,
            dma((5,)),
        ],
        compiler_params=pltpu.CompilerParams(collective_id=0, has_side_effects=True, vmem_limit_bytes=24 << 20),
    )(
        *(
            pltpu.with_memory_space_constraint(a, pltpu.HBM)
            for a in (tokens, proj_in, proj_out.T, jnp.asarray(chan, BF), jnp.asarray(first, BF), jnp.asarray(twist, F32), jnp.asarray(last, BF))
        )
    )
    return pl.pallas_call(
        product,
        out_shape=jax.ShapeDtypeStruct((1, LOC, D), BF),
        in_specs=[pl.BlockSpec(memory_space=pltpu.VMEM)] * 2,
        out_specs=pl.BlockSpec(memory_space=pl.ANY),
        scratch_shapes=[pltpu.VMEM((LOC, D), BF), dma((8,))],
        compiler_params=pltpu.CompilerParams(vmem_limit_bytes=24 << 20),
    )(lhs, pt)


def solution(mesh):
    return jax.shard_map(
        shards,
        mesh=mesh,
        in_specs=(P("col", "row", None), P("col", None), P(None, "row")),
        out_specs=P("col", "row", None),
        check_vma=False,
    )
```

```python
import math

import jax
import jax.numpy as jnp
import numpy as np
from jax import lax
from jax.experimental import pallas as pl
from jax.experimental.pallas import tpu as pltpu
from jax.sharding import PartitionSpec as P

MESH = pl.DeviceIdType.MESH
GRP = 128
GROUPS = 4
NZ, NY, NX = 16, 4, 4
ROWS = NZ * NY
LOC = 192
LEN = ROWS * LOC
D = 2048
KS = 256
FW = GROUPS * GRP
F32 = jnp.float32
BF = jnp.bfloat16


def tables():
    s = np.arange(64)[:, None]
    f = np.arange(GRP)[None, :]
    ang = 2 * np.pi * ((s * f) % GRP) / GRP
    part_a = np.cos(ang)
    part_b = np.sin(ang)
    part_b[0] = np.cos(np.pi * np.arange(GRP))
    chan = np.concatenate([part_a, part_b], 1)
    q = np.arange(LOC)[:, None]
    halves = []
    for e in range(2):
        p1 = np.array([3 * (NY * zz + e + 2 * h) + m for h in range(2) for zz in range(NZ) for m in range(3)])[None, :]
        ang = 2 * np.pi * ((q * p1) % LOC) / LOC
        halves.append(np.repeat(np.concatenate([np.cos(ang), np.sin(ang)], 0), 4, axis=1))
    first = np.stack(halves)
    q2 = np.arange(64)[None, :]
    ang = 2 * np.pi * ((q * q2) % LEN) / LEN
    scale = 1.0 / math.sqrt(GRP * LEN)
    twist = np.stack([np.tile(np.cos(ang), (1, 2)), np.tile(np.sin(ang), (1, 2))]) * scale
    r = np.arange(64)[:, None]
    ang = 2 * np.pi * ((r * q2) % 64) / 64
    c, n = np.cos(ang), np.sin(ang)
    last = np.repeat(np.concatenate([c, n, -n, c], 1), 4, axis=0)
    return chan, first, twist, last


def bdot(a, b):
    return lax.dot_general(a, b, (((1,), (1,)), ((), ())), preferred_element_type=F32)


def kernel(tok_hbm, win_hbm, pout_hbm, chan_hbm, first_hbm, twist_hbm, last_hbm, lhs_ref, pt, tok, wfull, pblk, chan, first, twist, last, m1, l3, blk, snd, acc, dat, snd2, dat2, ld, hops, w_s, pin_r, yin_r, ymt_r, a1_s, a1_r, a2_s, a2_r, pz_s, pz_r, p_s, py_r, px_r):
    row = lax.axis_index("row")
    col = lax.axis_index("col")
    z, y = row // NY, lax.rem(row, NY)
    x, core = col // 2, lax.rem(col, 2)
    xr = lax.rem(x + 1, NX)
    xl = lax.rem(x + NX - 1, NX)
    xo = lax.rem(x + 2, NX)
    right, left, mate = xr * 2 + core, xl * 2 + core, x * 2 + (1 - core)
    yu, yd, yo = lax.rem(y + 1, NY), lax.rem(y + NY - 1, NY), lax.rem(y + 2, NY)

    def at(dz, yy):
        return lax.rem(z + dz, NZ) * NY + yy

    bar = pltpu.get_barrier_semaphore()
    for peer in (right, left, xo * 2 + core, mate):
        pl.semaphore_signal(bar, inc=1, device_id={"col": peer}, device_id_type=MESH)
    for peer in (at(0, yu), at(0, yd), at(1, y), at(NZ - 1, y)):
        pl.semaphore_signal(bar, inc=1, device_id={"row": peer}, device_id_type=MESH)

    loads = [
        pltpu.make_async_copy(win_hbm, wfull.at[pl.ds(pl.multiple_of(col * KS, KS), KS), :], ld.at[0]),
        pltpu.make_async_copy(pout_hbm, pblk, ld.at[1]),
        pltpu.make_async_copy(tok_hbm.at[0], tok, ld.at[2]),
        pltpu.make_async_copy(chan_hbm, chan, ld.at[3]),
        pltpu.make_async_copy(first_hbm, first, ld.at[3]),
        pltpu.make_async_copy(last_hbm, last, ld.at[3]),
        pltpu.make_async_copy(twist_hbm, twist, ld.at[3]),
    ]
    for c in loads:
        c.start()
    pl.semaphore_wait(bar, 8)

    def tell(i, peers):
        for peer in peers:
            pl.semaphore_signal(hops.at[i], inc=1, device_id={"row": peer}, device_id_type=MESH)

    tell(0, (at(1, y), at(NZ - 1, y), at(0, yu), at(0, yd)))
    loads[0].wait()

    same = [col, xl * 2 + core, xr * 2 + core, xo * 2 + core]

    def tile(c, g):
        return wfull.at[pl.ds(pl.multiple_of(c * KS, KS), KS), pl.ds(pl.multiple_of(g * GRP, GRP), GRP)]

    def arrived(rows, sem):
        pltpu.make_async_copy(wfull.at[pl.ds(0, rows)], wfull.at[pl.ds(0, rows)], sem).wait()

    def push(ref, ss, rs, peer):
        return pltpu.make_async_remote_copy(src_ref=ref, dst_ref=ref, send_sem=ss, recv_sem=rs, device_id=peer, device_id_type=MESH)

    order = (y, yo, yu, yd)

    def along_x(t, k):
        return push(tile(col, order[t]), w_s, pin_r.at[k if t == 0 else 3], {"col": (right, left, xo * 2 + core)[k]})

    def to_mate(t, k):
        push(tile(same[k], order[t]), w_s, ymt_r.at[t], {"col": mate}).start()

    def along_y(d, k):
        push(tile(same[k], y), w_s, yin_r.at[k // 3], {"row": at(0, (yu, yd)[d])}).start()

    for k in range(3):
        along_x(0, k).start()
    to_mate(0, 0)

    @pl.when(core == 0)
    def _():
        for j in range(3):
            along_x(1, j).start()


    rid = lax.broadcasted_iota(jnp.int32, (FW, FW), 1)
    fid = lax.broadcasted_iota(jnp.int32, (FW, FW), 0)
    inner = lax.rem(rid, 256)
    slot = (inner // 16) * 4 + lax.rem(inner, 4)
    upper = jnp.where(slot == 0, 64, GRP - slot)
    want = lax.rem(inner // 4, 4) * GRP + jnp.where(rid < 256, slot, upper)
    perm = jnp.where(fid == want, 1.0, 0.0).astype(BF)
    loads[1].wait()
    blk[...] = jnp.dot(pblk[...], perm, preferred_element_type=F32).astype(BF)

    half = pl.ds(pl.multiple_of(core * 16, 16), 16)
    quarter = pl.ds(pl.multiple_of(x * GRP, GRP), GRP)

    def mine(yy, c=None):
        c = col if c is None else c
        return pt.at[yy, :, pl.ds(pl.multiple_of(lax.rem(c, 2) * 16, 16), 16), pl.ds(pl.multiple_of((c // 2) * GRP, GRP), GRP)]

    own = pltpu.make_async_copy(blk.at[half, quarter], pt.at[y, z, half, quarter], ld.at[4])
    own.start()

    def pz_send(dz):
        rs = pz_r.at[{4: 1, 12: 2}.get(dz, 0)]
        pltpu.make_async_remote_copy(src_ref=blk.at[half, quarter], dst_ref=pt.at[y, z, half, quarter], send_sem=pz_s, recv_sem=rs, device_id={"row": at(dz, y)}, device_id_type=MESH).start()

    def pz_relay(i):
        ref = pt.at[y, lax.rem(z + (12, 4)[i], NZ), half, quarter]
        pltpu.make_async_copy(ref, ref, pz_r.at[i + 1]).wait()
        for dz in ((3, 2, 1), (12, 13, 14, 15))[i]:
            push(ref, pz_s, pz_r.at[0], {"row": at(dz, y)}).start()

    pl.semaphore_wait(hops.at[0], 4)
    tell(1, (at(2, y), at(NZ - 2, y)))
    for dz in (1, 15, 2, 14):
        pz_send(dz)

    arrived(928, ld.at[3])
    lane = lax.rem(lax.broadcasted_iota(jnp.int32, (2 * LOC, 2 * LOC), 1), 4)
    sub = lax.rem(lax.broadcasted_iota(jnp.int32, (256, 256), 0), 4)
    for s in range(4):
        for e in range(2):
            m1[e, s] = first[e] * jnp.where(lane == s, 1.0, 0.0).astype(BF)
        l3[s] = last[...] * jnp.where(sub == s, 1.0, 0.0).astype(BF)

    pl.semaphore_wait(hops.at[1], 2)
    tell(2, (at(4, y), at(NZ - 4, y)))
    for dz in (3, 13, 4, 12):
        pz_send(dz)

    for k in range(3):
        arrived(64, pin_r.at[k])
        to_mate(0, k + 1)
        along_y(0, k + 1)
        along_y(1, k + 1)
        if k == 2:
            for t in range(1, 4):
                to_mate(t, 0)

            @pl.when(core == 1)
            def _():
                for j in range(3):
                    along_x(1, j).start()


    pl.semaphore_wait(hops.at[2], 2)
    tell(3, (at(0, yu), at(0, yd), at(0, yo)))
    own.wait()
    loads[2].wait()

    def pass_x():
        arrived(192, pin_r.at[3])
        for k in (1, 2, 3):
            to_mate(1, k)

    pl.when(core == 0)(pass_x)
    for i in range(2):
        pz_relay(i)

    def far(i):
        step = (i + 1) // 2
        return lax.rem(8 + step * (1 - 2 * lax.rem(i, 2)) + NZ, NZ)

    def px(u, k):
        c = (col, col, col, col, xl * 2 + core, xr * 2 + core, xo * 2 + core)[k]
        peer = (right, left, xo * 2 + core, mate, mate, mate, mate)[k]
        push(mine(order[u], c), p_s, px_r.at[u if k < 3 else 4], {"col": peer}).start()

    def px_out(u):
        for k in range(4):
            px(u, k)

    side = lax.rem(y, 2)

    def groups_out(t, which):
        def send():
            def a1_send(i, c):
                to = lax.rem(z + far(i), NZ)
                pltpu.make_async_remote_copy(src_ref=snd.at[t, to], dst_ref=dat.at[side, y // 2, z], send_sem=a1_s, recv_sem=a1_r.at[t // 2], device_id={"row": to * NY + order[t]}, device_id_type=MESH).start()
                return c

            lax.fori_loop(0, NZ - 1 if t == 0 else NZ, a1_send, 0)
            if t == 0:
                pltpu.make_async_copy(snd.at[0, z], dat.at[side, y // 2, z], a1_r.at[0]).start()

        if which is None:
            send()
        else:
            pl.when(core == which)(send)

    for t in range(GROUPS):
        g = order[t]
        if t == 1:
            pl.semaphore_wait(hops.at[3], 3)
            pl.when(core == 1)(pass_x)
            arrived(256, yin_r.at[0])
            for k in (1, 2):
                to_mate(2, k)
                to_mate(3, k)
        if t == 2:
            arrived(128, yin_r.at[1])
            to_mate(2, 3)
            to_mate(3, 3)
            part = pt.at[y, pl.ds(0, NZ - 3), half, quarter]
            pltpu.make_async_copy(part, part, pz_r.at[0]).wait()
            for o in range(3):
                push(mine(y), p_s, py_r, {"row": at(0, order[o + 1])}).start()
            px_out(0)
        arrived(256, ymt_r.at[t])
        w = wfull[:, pl.ds(pl.multiple_of(g * GRP, GRP), GRP)]
        mapped = jnp.dot(tok[...], w, preferred_element_type=F32).astype(BF)
        zero = jnp.zeros((64, GRP), BF)
        parts = []
        for m in range(3):
            piece = mapped[64 * m : 64 * m + 64]
            parts.append(jnp.concatenate([piece, zero], 1))
            parts.append(jnp.concatenate([zero, piece], 1))
        spread = bdot(chan[...], jnp.concatenate(parts, 0))
        for m in range(3):
            snd[t, :, m] = spread[:, GRP * m : GRP * m + GRP].reshape(NZ, 4, GRP).astype(BF)

        for u in range(GROUPS):
            early, late = u == t, t == min(u + 1, GROUPS - 1)
            if early or late:
                which = None if early and late else 1 if early else 0
                groups_out(u, which)

    arrived(192, py_r)
    for u in (1, 2, 3):
        px_out(u)

    early = dat.at[side]
    pltpu.make_async_copy(early, early, a1_r.at[0]).wait()
    data = early[...].reshape(2 * LOC, GRP)
    for s in range(4):
        acc[s] = jnp.dot(m1[side, s], data, preferred_element_type=F32)
    late = dat.at[1 - side]
    pltpu.make_async_copy(late, late, a1_r.at[1]).wait()
    data = late[...].reshape(2 * LOC, GRP)
    cc, sn = twist[0], twist[1]
    first_slot = z == 0
    lanes = lax.broadcasted_iota(jnp.int32, (1, GRP), 1) < 64
    sgn = jnp.where(lanes, 1.0, -1.0)
    zero_b = jnp.where(lanes, 1.0, 0.0)
    spec = jnp.where(first_slot, 1.0, 0.0)
    outs = [None] * 3
    for s in range(4):
        got = acc[s] + jnp.dot(m1[1 - side, s], data, preferred_element_type=F32)
        re, im = got[:LOC], got[LOC:]
        tre = re * cc - im * sn
        tim = re * sn + im * cc
        if s == 0:
            lo_mask = zero_b * spec + sgn * (1.0 - spec)
            up_keep, up_turn = 1.0 - spec, zero_b * spec
            lo_re, lo_im = tre * lo_mask, tim * lo_mask
            up_re = tre * up_keep + pltpu.roll(tre, 64, 1) * up_turn
            up_im = tim * up_keep + pltpu.roll(tim, 64, 1) * up_turn
        else:
            lo_re, lo_im, up_re, up_im = tre * sgn, tim * sgn, tre, tim
        lo = jnp.concatenate([lo_re, lo_im], 1).astype(BF)
        up = jnp.concatenate([up_re, up_im], 1).astype(BF)
        for m in range(3):
            rhs = jnp.concatenate([lo[64 * m : 64 * m + 64], up[64 * m : 64 * m + 64]], 0)
            term = bdot(l3[s], rhs)
            outs[m] = term if outs[m] is None else outs[m] + term
    for m in range(3):
        snd2[:, m] = outs[m].reshape(ROWS, 4, GRP).astype(BF)

    pltpu.make_async_copy(snd2.at[row], dat2.at[row], a2_r).start()

    def a2_send(i, c):
        to = at(far(i // NY), lax.rem(y + lax.rem(i + 1, NY), NY))
        pltpu.make_async_remote_copy(src_ref=snd2.at[to], dst_ref=dat2.at[row], send_sem=a2_s, recv_sem=a2_r, device_id={"row": to}, device_id_type=MESH).start()
        return c

    lax.fori_loop(0, ROWS - 1, a2_send, 0)

    for u in range(4):
        arrived(192, px_r.at[u])
        for k in (4, 5, 6):
            px(u, k)

    arrived(28 * 64, w_s)
    part = pt.at[y, pl.ds(0, NZ - 1), half, quarter]
    pltpu.make_async_copy(part, part, pz_s).wait()
    arrived(31 * 64, p_s)
    for sem in (a1_s, a2_s):
        pltpu.make_async_copy(dat2.at[pl.ds(0, ROWS - 1)], dat2.at[pl.ds(0, ROWS - 1)], sem).wait()
    arrived(1024, px_r.at[4])

    pltpu.make_async_copy(dat2, dat2, a2_r).wait()
    sides = []
    for m in range(3):
        t = dat2[:, m].reshape(256, GRP).T
        sides.append(jnp.concatenate([t[:64], t[64:]], 1))
    lhs = jnp.concatenate(sides, 0)
    lhs_ref[...] = lhs


def product(lhs_ref, pt_ref, out_hbm, out, sem):
    wide = D // 8
    copies = []
    for n in range(8):
        cols = pl.ds(wide * n, wide)
        rhs = jnp.concatenate([pt_ref[yy, zz] for zz in (2 * n, 2 * n + 1) for yy in range(NY)], 0)
        out[:, cols] = bdot(lhs_ref[...], rhs).astype(BF)
        copies.append(pltpu.make_async_copy(out.at[:, cols], out_hbm.at[0, :, cols], sem.at[n]))
        copies[-1].start()
    for c in copies:
        c.wait()


def shards(tokens, proj_in, proj_out):
    chan, first, twist, last = tables()
    anyspec = pl.BlockSpec(memory_space=pltpu.HBM)
    dma = pltpu.SemaphoreType.DMA
    lhs, pt = pl.pallas_call(
        kernel,
        out_shape=(jax.ShapeDtypeStruct((LOC, FW), BF), jax.ShapeDtypeStruct((NY, NZ, 32, FW), BF)),
        in_specs=[anyspec] * 7,
        out_specs=(pl.BlockSpec(memory_space=pltpu.VMEM), pl.BlockSpec(memory_space=pltpu.VMEM)),
        scratch_shapes=[
            pltpu.VMEM((LOC, D), BF),
            pltpu.VMEM((D, FW), BF),
            pltpu.VMEM((32, FW), BF),
            pltpu.VMEM((64, 256), BF),
            pltpu.VMEM((2, 2 * LOC, 2 * LOC), BF),
            pltpu.VMEM((2, LOC, GRP), F32),
            pltpu.VMEM((256, 256), BF),
            pltpu.VMEM((2, 4, 2 * LOC, 2 * LOC), BF),
            pltpu.VMEM((4, 256, 256), BF),
            pltpu.VMEM((32, FW), BF),
            pltpu.VMEM((GROUPS, NZ, 3, 4, GRP), BF),
            pltpu.VMEM((4, 2 * LOC, GRP), F32),
            pltpu.VMEM((2, 2, NZ, 3, 4, GRP), BF),
            pltpu.VMEM((ROWS, 3, 4, GRP), BF),
            pltpu.VMEM((ROWS, 3, 4, GRP), BF),
            dma((5,)),
            pltpu.SemaphoreType.REGULAR((4,)),
            dma,
            dma((4,)),
            dma((2,)),
            dma((4,)),
            dma,
            dma((2,)),
            dma,
            dma,
            dma,
            dma((3,)),
            dma,
            dma,
            dma((5,)),
        ],
        compiler_params=pltpu.CompilerParams(collective_id=0, has_side_effects=True, vmem_limit_bytes=24 << 20),
    )(
        *(
            pltpu.with_memory_space_constraint(a, pltpu.HBM)
            for a in (tokens, proj_in, proj_out.T, jnp.asarray(chan, BF), jnp.asarray(first, BF), jnp.asarray(twist, F32), jnp.asarray(last, BF))
        )
    )
    return pl.pallas_call(
        product,
        out_shape=jax.ShapeDtypeStruct((1, LOC, D), BF),
        in_specs=[pl.BlockSpec(memory_space=pltpu.VMEM)] * 2,
        out_specs=pl.BlockSpec(memory_space=pl.ANY),
        scratch_shapes=[pltpu.VMEM((LOC, D), BF), dma((8,))],
        compiler_params=pltpu.CompilerParams(vmem_limit_bytes=24 << 20),
    )(lhs, pt)


def solution(mesh):
    return jax.shard_map(
        shards,
        mesh=mesh,
        in_specs=(P("col", "row", None), P("col", None), P(None, "row")),
        out_specs=P("col", "row", None),
        check_vma=False,
    )
```

```python
import math

import jax
import jax.numpy as jnp
import numpy as np
from jax import lax
from jax.experimental import pallas as pl
from jax.experimental.pallas import tpu as pltpu
from jax.sharding import PartitionSpec as P

MESH = pl.DeviceIdType.MESH
GRP = 128
GROUPS = 4
NZ, NY, NX = 16, 4, 4
ROWS = NZ * NY
LOC = 192
LEN = ROWS * LOC
D = 2048
KS = 256
FW = GROUPS * GRP
F32 = jnp.float32
BF = jnp.bfloat16


def tables():
    s = np.arange(64)[:, None]
    f = np.arange(GRP)[None, :]
    ang = 2 * np.pi * ((s * f) % GRP) / GRP
    part_a = np.cos(ang)
    part_b = np.sin(ang)
    part_b[0] = np.cos(np.pi * np.arange(GRP))
    chan = np.concatenate([part_a, part_b], 1)
    q = np.arange(LOC)[:, None]
    halves = []
    for e in range(2):
        p1 = np.array([3 * (NY * zz + e + 2 * h) + m for h in range(2) for zz in range(NZ) for m in range(3)])[None, :]
        ang = 2 * np.pi * ((q * p1) % LOC) / LOC
        halves.append(np.repeat(np.concatenate([np.cos(ang), np.sin(ang)], 0), 4, axis=1))
    first = np.stack(halves)
    q2 = np.arange(64)[None, :]
    ang = 2 * np.pi * ((q * q2) % LEN) / LEN
    scale = 1.0 / math.sqrt(GRP * LEN)
    twist = np.stack([np.tile(np.cos(ang), (1, 2)), np.tile(np.sin(ang), (1, 2))]) * scale
    r = np.arange(64)[:, None]
    ang = 2 * np.pi * ((r * q2) % 64) / 64
    c, n = np.cos(ang), np.sin(ang)
    last = np.repeat(np.concatenate([c, n, -n, c], 1), 4, axis=0)
    return chan, first, twist, last


def bdot(a, b):
    return lax.dot_general(a, b, (((1,), (1,)), ((), ())), preferred_element_type=F32)


def kernel(tok_hbm, win_hbm, pout_hbm, chan_hbm, first_hbm, twist_hbm, last_hbm, lhs_ref, pt, tok, wfull, pblk, chan, first, twist, last, m1, l3, blk, snd, acc, dat, snd2, dat2, ld, hops, w_s, pin_r, yin_r, ymt_r, a1_s, a1_r, a2_s, a2_r, pz_s, pz_r, p_s, py_r, px_r):
    row = lax.axis_index("row")
    col = lax.axis_index("col")
    z, y = row // NY, lax.rem(row, NY)
    x, core = col // 2, lax.rem(col, 2)
    xr = lax.rem(x + 1, NX)
    xl = lax.rem(x + NX - 1, NX)
    xo = lax.rem(x + 2, NX)
    right, left, mate = xr * 2 + core, xl * 2 + core, x * 2 + (1 - core)
    yu, yd, yo = lax.rem(y + 1, NY), lax.rem(y + NY - 1, NY), lax.rem(y + 2, NY)

    def at(dz, yy):
        return lax.rem(z + dz, NZ) * NY + yy

    bar = pltpu.get_barrier_semaphore()
    for peer in (right, left, xo * 2 + core, mate):
        pl.semaphore_signal(bar, inc=1, device_id={"col": peer}, device_id_type=MESH)
    for peer in (at(0, yu), at(0, yd), at(1, y), at(NZ - 1, y)):
        pl.semaphore_signal(bar, inc=1, device_id={"row": peer}, device_id_type=MESH)

    loads = [
        pltpu.make_async_copy(win_hbm, wfull.at[pl.ds(pl.multiple_of(col * KS, KS), KS), :], ld.at[0]),
        pltpu.make_async_copy(pout_hbm, pblk, ld.at[1]),
        pltpu.make_async_copy(tok_hbm.at[0], tok, ld.at[2]),
        pltpu.make_async_copy(chan_hbm, chan, ld.at[3]),
        pltpu.make_async_copy(first_hbm, first, ld.at[3]),
        pltpu.make_async_copy(last_hbm, last, ld.at[3]),
        pltpu.make_async_copy(twist_hbm, twist, ld.at[3]),
    ]
    for c in loads:
        c.start()
    pl.semaphore_wait(bar, 8)

    def tell(i, peers):
        for peer in peers:
            pl.semaphore_signal(hops.at[i], inc=1, device_id={"row": peer}, device_id_type=MESH)

    tell(0, (at(1, y), at(NZ - 1, y), at(0, yu), at(0, yd)))
    loads[0].wait()

    same = [col, xl * 2 + core, xr * 2 + core, xo * 2 + core]

    def tile(c, g):
        return wfull.at[pl.ds(pl.multiple_of(c * KS, KS), KS), pl.ds(pl.multiple_of(g * GRP, GRP), GRP)]

    def arrived(rows, sem):
        pltpu.make_async_copy(wfull.at[pl.ds(0, rows)], wfull.at[pl.ds(0, rows)], sem).wait()

    def push(ref, ss, rs, peer):
        return pltpu.make_async_remote_copy(src_ref=ref, dst_ref=ref, send_sem=ss, recv_sem=rs, device_id=peer, device_id_type=MESH)

    order = (y, yo, yu, yd)

    def along_x(t, k):
        return push(tile(col, order[t]), w_s, pin_r.at[k if t == 0 else 3], {"col": (right, left, xo * 2 + core)[k]})

    def to_mate(t, k):
        push(tile(same[k], order[t]), w_s, ymt_r.at[t], {"col": mate}).start()

    def along_y(d, k):
        push(tile(same[k], y), w_s, yin_r.at[k // 3], {"row": at(0, (yu, yd)[d])}).start()

    for k in range(3):
        along_x(0, k).start()
    to_mate(0, 0)

    @pl.when(core == 0)
    def _():
        for j in range(3):
            along_x(1, j).start()


    rid = lax.broadcasted_iota(jnp.int32, (FW, FW), 1)
    fid = lax.broadcasted_iota(jnp.int32, (FW, FW), 0)
    inner = lax.rem(rid, 256)
    slot = (inner // 16) * 4 + lax.rem(inner, 4)
    upper = jnp.where(slot == 0, 64, GRP - slot)
    want = lax.rem(inner // 4, 4) * GRP + jnp.where(rid < 256, slot, upper)
    perm = jnp.where(fid == want, 1.0, 0.0).astype(BF)
    loads[1].wait()
    blk[...] = jnp.dot(pblk[...], perm, preferred_element_type=F32).astype(BF)

    half = pl.ds(pl.multiple_of(core * 16, 16), 16)
    quarter = pl.ds(pl.multiple_of(x * GRP, GRP), GRP)

    def mine(yy, c=None):
        c = col if c is None else c
        return pt.at[yy, :, pl.ds(pl.multiple_of(lax.rem(c, 2) * 16, 16), 16), pl.ds(pl.multiple_of((c // 2) * GRP, GRP), GRP)]

    own = pltpu.make_async_copy(blk.at[half, quarter], pt.at[y, z, half, quarter], ld.at[4])
    own.start()

    def pz_send(dz):
        rs = pz_r.at[{4: 1, 12: 2}.get(dz, 0)]
        pltpu.make_async_remote_copy(src_ref=blk.at[half, quarter], dst_ref=pt.at[y, z, half, quarter], send_sem=pz_s, recv_sem=rs, device_id={"row": at(dz, y)}, device_id_type=MESH).start()

    def pz_relay(i):
        ref = pt.at[y, lax.rem(z + (12, 4)[i], NZ), half, quarter]
        pltpu.make_async_copy(ref, ref, pz_r.at[i + 1]).wait()
        for dz in ((3, 2, 1), (12, 13, 14, 15))[i]:
            push(ref, pz_s, pz_r.at[0], {"row": at(dz, y)}).start()

    pl.semaphore_wait(hops.at[0], 4)
    tell(1, (at(2, y), at(NZ - 2, y)))
    for dz in (1, 15, 2, 14):
        pz_send(dz)

    arrived(928, ld.at[3])
    lane = lax.rem(lax.broadcasted_iota(jnp.int32, (2 * LOC, 2 * LOC), 1), 4)
    sub = lax.rem(lax.broadcasted_iota(jnp.int32, (256, 256), 0), 4)
    for s in range(4):
        for e in range(2):
            m1[e, s] = first[e] * jnp.where(lane == s, 1.0, 0.0).astype(BF)
        l3[s] = last[...] * jnp.where(sub == s, 1.0, 0.0).astype(BF)

    pl.semaphore_wait(hops.at[1], 2)
    tell(2, (at(4, y), at(NZ - 4, y)))
    for dz in (3, 13, 4, 12):
        pz_send(dz)

    for k in range(3):
        arrived(64, pin_r.at[k])
        to_mate(0, k + 1)
        along_y(0, k + 1)
        along_y(1, k + 1)
        if k == 2:
            for t in range(1, 4):
                to_mate(t, 0)

            @pl.when(core == 1)
            def _():
                for j in range(3):
                    along_x(1, j).start()


    pl.semaphore_wait(hops.at[2], 2)
    tell(3, (at(0, yu), at(0, yd), at(0, yo)))
    own.wait()
    loads[2].wait()

    def pass_x():
        arrived(192, pin_r.at[3])
        for k in (1, 2, 3):
            to_mate(1, k)

    def pass_y():
        arrived(256, yin_r.at[0])
        for k in (1, 2):
            to_mate(2, k)
            to_mate(3, k)

    pl.when(core == 0)(pass_x)
    for i in range(2):
        pz_relay(i)
    pl.when(core == 0)(pass_y)

    def far(i):
        step = (i + 1) // 2
        return lax.rem(8 + step * (1 - 2 * lax.rem(i, 2)) + NZ, NZ)

    def px(u, k):
        c = (col, col, col, col, xl * 2 + core, xr * 2 + core, xo * 2 + core)[k]
        peer = (right, left, xo * 2 + core, mate, mate, mate, mate)[k]
        push(mine(order[u], c), p_s, px_r.at[u if k < 3 else 4], {"col": peer}).start()

    def px_out(u):
        for k in range(4):
            px(u, k)

    side = lax.rem(y, 2)

    def groups_out(t, which):
        def send():
            def a1_send(i, c):
                to = lax.rem(z + far(i), NZ)
                pltpu.make_async_remote_copy(src_ref=snd.at[t, to], dst_ref=dat.at[side, y // 2, z], send_sem=a1_s, recv_sem=a1_r.at[t // 2], device_id={"row": to * NY + order[t]}, device_id_type=MESH).start()
                return c

            lax.fori_loop(0, NZ - 1 if t == 0 else NZ, a1_send, 0)
            if t == 0:
                pltpu.make_async_copy(snd.at[0, z], dat.at[side, y // 2, z], a1_r.at[0]).start()

        if which is None:
            send()
        else:
            pl.when(core == which)(send)

    for t in range(GROUPS):
        g = order[t]
        if t == 1:
            pl.semaphore_wait(hops.at[3], 3)
            pl.when(core == 1)(pass_x)
            pl.when(core == 1)(pass_y)
        if t == 2:
            arrived(128, yin_r.at[1])
            to_mate(2, 3)
            to_mate(3, 3)
            part = pt.at[y, pl.ds(0, NZ - 3), half, quarter]
            pltpu.make_async_copy(part, part, pz_r.at[0]).wait()
            for o in range(3):
                push(mine(y), p_s, py_r, {"row": at(0, order[o + 1])}).start()
            px_out(0)
        arrived(256, ymt_r.at[t])
        w = wfull[:, pl.ds(pl.multiple_of(g * GRP, GRP), GRP)]
        mapped = jnp.dot(tok[...], w, preferred_element_type=F32).astype(BF)
        zero = jnp.zeros((64, GRP), BF)
        parts = []
        for m in range(3):
            piece = mapped[64 * m : 64 * m + 64]
            parts.append(jnp.concatenate([piece, zero], 1))
            parts.append(jnp.concatenate([zero, piece], 1))
        spread = bdot(chan[...], jnp.concatenate(parts, 0))
        for m in range(3):
            snd[t, :, m] = spread[:, GRP * m : GRP * m + GRP].reshape(NZ, 4, GRP).astype(BF)

        for u in range(GROUPS):
            early, late = u == t, t == min(u + 1, GROUPS - 1)
            if early or late:
                which = None if early and late else 1 if early else 0
                groups_out(u, which)

    arrived(192, py_r)
    for u in (1, 2, 3):
        px_out(u)

    early = dat.at[side]
    pltpu.make_async_copy(early, early, a1_r.at[0]).wait()
    data = early[...].reshape(2 * LOC, GRP)
    for s in range(4):
        acc[s] = jnp.dot(m1[side, s], data, preferred_element_type=F32)
    late = dat.at[1 - side]
    pltpu.make_async_copy(late, late, a1_r.at[1]).wait()
    data = late[...].reshape(2 * LOC, GRP)
    cc, sn = twist[0], twist[1]
    first_slot = z == 0
    lanes = lax.broadcasted_iota(jnp.int32, (1, GRP), 1) < 64
    sgn = jnp.where(lanes, 1.0, -1.0)
    zero_b = jnp.where(lanes, 1.0, 0.0)
    spec = jnp.where(first_slot, 1.0, 0.0)
    outs = [None] * 3
    for s in range(4):
        got = acc[s] + jnp.dot(m1[1 - side, s], data, preferred_element_type=F32)
        re, im = got[:LOC], got[LOC:]
        tre = re * cc - im * sn
        tim = re * sn + im * cc
        if s == 0:
            lo_mask = zero_b * spec + sgn * (1.0 - spec)
            up_keep, up_turn = 1.0 - spec, zero_b * spec
            lo_re, lo_im = tre * lo_mask, tim * lo_mask
            up_re = tre * up_keep + pltpu.roll(tre, 64, 1) * up_turn
            up_im = tim * up_keep + pltpu.roll(tim, 64, 1) * up_turn
        else:
            lo_re, lo_im, up_re, up_im = tre * sgn, tim * sgn, tre, tim
        lo = jnp.concatenate([lo_re, lo_im], 1).astype(BF)
        up = jnp.concatenate([up_re, up_im], 1).astype(BF)
        for m in range(3):
            rhs = jnp.concatenate([lo[64 * m : 64 * m + 64], up[64 * m : 64 * m + 64]], 0)
            term = bdot(l3[s], rhs)
            outs[m] = term if outs[m] is None else outs[m] + term
    for m in range(3):
        snd2[:, m] = outs[m].reshape(ROWS, 4, GRP).astype(BF)

    pltpu.make_async_copy(snd2.at[row], dat2.at[row], a2_r).start()

    def a2_send(i, c):
        to = at(far(i // NY), lax.rem(y + lax.rem(i + 1, NY), NY))
        pltpu.make_async_remote_copy(src_ref=snd2.at[to], dst_ref=dat2.at[row], send_sem=a2_s, recv_sem=a2_r, device_id={"row": to}, device_id_type=MESH).start()
        return c

    lax.fori_loop(0, ROWS - 1, a2_send, 0)

    for u in range(4):
        arrived(192, px_r.at[u])
        for k in (4, 5, 6):
            px(u, k)

    arrived(28 * 64, w_s)
    part = pt.at[y, pl.ds(0, NZ - 1), half, quarter]
    pltpu.make_async_copy(part, part, pz_s).wait()
    arrived(31 * 64, p_s)
    for sem in (a1_s, a2_s):
        pltpu.make_async_copy(dat2.at[pl.ds(0, ROWS - 1)], dat2.at[pl.ds(0, ROWS - 1)], sem).wait()
    arrived(1024, px_r.at[4])

    pltpu.make_async_copy(dat2, dat2, a2_r).wait()
    sides = []
    for m in range(3):
        t = dat2[:, m].reshape(256, GRP).T
        sides.append(jnp.concatenate([t[:64], t[64:]], 1))
    lhs = jnp.concatenate(sides, 0)
    lhs_ref[...] = lhs


def product(lhs_ref, pt_ref, out_hbm, out, sem):
    wide = D // 8
    copies = []
    for n in range(8):
        cols = pl.ds(wide * n, wide)
        rhs = jnp.concatenate([pt_ref[yy, zz] for zz in (2 * n, 2 * n + 1) for yy in range(NY)], 0)
        out[:, cols] = bdot(lhs_ref[...], rhs).astype(BF)
        copies.append(pltpu.make_async_copy(out.at[:, cols], out_hbm.at[0, :, cols], sem.at[n]))
        copies[-1].start()
    for c in copies:
        c.wait()


def shards(tokens, proj_in, proj_out):
    chan, first, twist, last = tables()
    anyspec = pl.BlockSpec(memory_space=pltpu.HBM)
    dma = pltpu.SemaphoreType.DMA
    lhs, pt = pl.pallas_call(
        kernel,
        out_shape=(jax.ShapeDtypeStruct((LOC, FW), BF), jax.ShapeDtypeStruct((NY, NZ, 32, FW), BF)),
        in_specs=[anyspec] * 7,
        out_specs=(pl.BlockSpec(memory_space=pltpu.VMEM), pl.BlockSpec(memory_space=pltpu.VMEM)),
        scratch_shapes=[
            pltpu.VMEM((LOC, D), BF),
            pltpu.VMEM((D, FW), BF),
            pltpu.VMEM((32, FW), BF),
            pltpu.VMEM((64, 256), BF),
            pltpu.VMEM((2, 2 * LOC, 2 * LOC), BF),
            pltpu.VMEM((2, LOC, GRP), F32),
            pltpu.VMEM((256, 256), BF),
            pltpu.VMEM((2, 4, 2 * LOC, 2 * LOC), BF),
            pltpu.VMEM((4, 256, 256), BF),
            pltpu.VMEM((32, FW), BF),
            pltpu.VMEM((GROUPS, NZ, 3, 4, GRP), BF),
            pltpu.VMEM((4, 2 * LOC, GRP), F32),
            pltpu.VMEM((2, 2, NZ, 3, 4, GRP), BF),
            pltpu.VMEM((ROWS, 3, 4, GRP), BF),
            pltpu.VMEM((ROWS, 3, 4, GRP), BF),
            dma((5,)),
            pltpu.SemaphoreType.REGULAR((4,)),
            dma,
            dma((4,)),
            dma((2,)),
            dma((4,)),
            dma,
            dma((2,)),
            dma,
            dma,
            dma,
            dma((3,)),
            dma,
            dma,
            dma((5,)),
        ],
        compiler_params=pltpu.CompilerParams(collective_id=0, has_side_effects=True, vmem_limit_bytes=24 << 20),
    )(
        *(
            pltpu.with_memory_space_constraint(a, pltpu.HBM)
            for a in (tokens, proj_in, proj_out.T, jnp.asarray(chan, BF), jnp.asarray(first, BF), jnp.asarray(twist, F32), jnp.asarray(last, BF))
        )
    )
    return pl.pallas_call(
        product,
        out_shape=jax.ShapeDtypeStruct((1, LOC, D), BF),
        in_specs=[pl.BlockSpec(memory_space=pltpu.VMEM)] * 2,
        out_specs=pl.BlockSpec(memory_space=pl.ANY),
        scratch_shapes=[pltpu.VMEM((LOC, D), BF), dma((8,))],
        compiler_params=pltpu.CompilerParams(vmem_limit_bytes=24 << 20),
    )(lhs, pt)


def solution(mesh):
    return jax.shard_map(
        shards,
        mesh=mesh,
        in_specs=(P("col", "row", None), P("col", None), P(None, "row")),
        out_specs=P("col", "row", None),
        check_vma=False,
    )
```
